32 devices in a mesh: sp: 8 (over z, y), tp: 4 (over x, core).
Axes of the slice: x: 2, y: 2, z: 4, core: 2. Of those that a mesh axis runs over, the one named last changes fastest.
Arguments:
- layer_input_rows: bfloat16 [2048, 2048], P('sp'), may hold values from -6 to 6
- input_norm_gain: float32 [2048], replicated, may hold values from 0.1 to 1.9
- query_weight: bfloat16 [2048, 1024], P(None, 'tp'), may hold values from -0.125 to 0.125
- key_weight: bfloat16 [2048, 1024], P(None, 'tp'), may hold values from -0.125 to 0.125
- value_weight: bfloat16 [2048, 1024], P(None, 'tp'), may hold values from -0.125 to 0.125
- query_norm_gain: float32 [64], replicated, may hold values from 0.5 to 9
- key_norm_gain: float32 [64], replicated, may hold values from 0.5 to 9
- cumulative_gate: float32 [2048, 16], P('sp', 'tp'), may hold values from -288.72 to 0, as said below
- attention_norm_gain: float32 [1024], P('tp'), may hold values from 0.1 to 1.9
- recurrence_query_weight: bfloat16 [2048, 1024], P(None, 'tp'), may hold values from -0.125 to 0.125
- forget_weight: bfloat16 [2048, 1024], P(None, 'tp'), may hold values from -0.125 to 0.125
- recurrence_value_weight: bfloat16 [2048, 1024], P(None, 'tp'), may hold values from -0.125 to 0.125
- output_gate_weight: bfloat16 [2048, 1024], P(None, 'tp'), may hold values from -0.125 to 0.125
- gate_lower_slack: float32 [1024], P('tp'), may hold values from 0 to 0.06
- extra_log_decay: float32 [2048, 8], P('sp', 'tp'), may hold values from -1.5 to 0
- recurrence_norm_gain: float32 [1024], P('tp'), may hold values from 0.1 to 1.9
- attention_output_weight: bfloat16 [1024, 2048], P('tp'), may hold values from -0.125 to 0.125
- recurrence_output_weight: bfloat16 [1024, 2048], P('tp'), may hold values from -0.125 to 0.125
Outputs:
- mixed: bfloat16 [2048, 2048], P(('sp', 'tp'))
- log_sum: float32 [2048, 16], P('sp', 'tp')
The draws below stay inside these ranges and needn't reach their ends.
Inputs may be any that keep to these rules, and one draw needn't show every extreme that they name: `cumulative_gate`: each column never rises along positions.
All inputs are finite; a program needn't handle non-finite values.
Results may differ from the reference program's by a relative error of at most 0.015.
The reference program's roundings to bfloat16 on the way count: a program that leaves them out, or rounds other values in their place, can miss the bound.
Values may be sent and summed in bfloat16 or wider, within the bound.
A program may use at most 64 MiB of HBM per device.

```python
import math
import jax
import jax.numpy as jnp
from jax import lax

D = 2048
ATT_HEADS = 16
HEAD_DIM = 64
RECURRENCE_HEADS = 8
STATE_ROWS = 128
VAL_DIM = 128
BLOCK = 64
TOKEN_COUNT = 2048
N_TP = 4


def gain_draw(base_key, salt_value):
    subkey = jax.random.fold_in(base_key, salt_value)
    return 1.0 + 0.18 * jax.random.truncated_normal(subkey, -2.5, 2.5, (HEAD_DIM,), jnp.float32)


def draw_query_norm_gain(key, part):
    return gain_draw(key, 11)


def draw_key_norm_gain(key, part):
    return gain_draw(key, 12)


def rough_logs(base_key, head_number, rates):
    random_subkeys = jax.random.split(base_key, 4)
    position_index = jnp.arange(TOKEN_COUNT, dtype=jnp.int32)
    block_of = position_index * 32 // TOKEN_COUNT
    factors = jnp.exp(jax.random.uniform(random_subkeys[0], (32, head_number), jnp.float32, -0.7, 0.7))
    block_scale = jnp.take(factors, block_of, axis=0)
    roughness = jax.random.uniform(random_subkeys[1], (TOKEN_COUNT, head_number), jnp.float32, 0.0, 2.0)
    logit_values = -rates[None, :] * block_scale * roughness
    spike_position = jax.random.randint(random_subkeys[2], (2, head_number), 0, TOKEN_COUNT)
    spike_depth = jnp.log(jax.random.uniform(random_subkeys[3], (2, head_number), jnp.float32, 0.5, 0.8))
    spike_hits = (position_index[:, None, None] == spike_position[None]).astype(jnp.float32)
    return logit_values + jnp.sum(spike_hits * spike_depth[None], axis=1)


def draw_cumulative_gate(key, part):
    random_subkeys = jax.random.split(jax.random.fold_in(key, 21), 4)
    ranking = jax.random.permutation(random_subkeys[0], ATT_HEADS)
    fast_count = ATT_HEADS // 2
    slow_heads = ranking >= fast_count
    slow_rate = jnp.exp(jax.random.uniform(random_subkeys[1], (ATT_HEADS,), jnp.float32, -0.69, 0.69)) / TOKEN_COUNT
    fast_rate = jnp.exp(jax.random.uniform(random_subkeys[2], (ATT_HEADS,), jnp.float32, -4.6, -3.4))
    rates = jnp.where(slow_heads, slow_rate, fast_rate)
    return jnp.cumsum(rough_logs(random_subkeys[3], ATT_HEADS, rates), axis=0)


def draw_extra_log_decay(key, part):
    random_subkeys = jax.random.split(jax.random.fold_in(key, 31), 2)
    rates = jnp.exp(jax.random.uniform(random_subkeys[0], (RECURRENCE_HEADS,), jnp.float32, -2.3, -0.22)) / TOKEN_COUNT
    return rough_logs(random_subkeys[1], RECURRENCE_HEADS, rates)


def draw_gate_lower_slack(key, part):
    random_subkeys = jax.random.split(jax.random.fold_in(key, 41), 3)
    channels = RECURRENCE_HEADS * STATE_ROWS
    ranking = jax.random.permutation(random_subkeys[0], channels)
    fast_count = channels // 2
    slow_rows = ranking >= fast_count
    slow_gap = jnp.exp(jax.random.uniform(random_subkeys[1], (channels,), jnp.float32, -1.6, 0.0)) / TOKEN_COUNT
    fast_gap = jnp.exp(jax.random.uniform(random_subkeys[2], (channels,), jnp.float32, -3.9, -2.82))
    return jnp.where(slow_rows, slow_gap, fast_gap)


def steps_of(rng, shape, cuts, smallest, high):
    loudness = 1.0
    for axis_at, parts in cuts:
        steps = jax.random.uniform(jax.random.fold_in(jax.random.fold_in(rng, 6), axis_at), (parts,), jnp.float32, smallest / len(cuts), high / len(cuts))
        loudness = loudness * jnp.repeat(jnp.exp(steps), shape[axis_at] // parts).reshape((-1,) + (1,) * (len(shape) - 1 - axis_at))
    return loudness


def centred(own_key, extent, spread, limit, pieces=(), kind=jnp.bfloat16):
    level = steps_of(own_key, extent, pieces, -0.22, 0.18) if pieces else 1.0
    array = jax.random.normal(own_key, extent, jnp.float32) * spread * level
    return jnp.minimum(jnp.maximum(array, -limit), limit).astype(kind)


def setup_inputs(seed: int = 0) -> dict:
    arg_keys = jax.random.split(jax.random.key(seed), 19)
    return {
        "layer_input_rows": centred(arg_keys[0], (TOKEN_COUNT, D), 1.0, 6.0, ((0, 8),)),
        "input_norm_gain": jnp.clip(1.0 + 0.18 * jax.random.normal(arg_keys[1], (D,), jnp.float32), 0.1, 1.9),
        "query_weight": centred(arg_keys[2], (D, ATT_HEADS * HEAD_DIM), D ** -0.5, 0.125, ((1, 4),)),
        "key_weight": centred(arg_keys[3], (D, ATT_HEADS * HEAD_DIM), D ** -0.5, 0.125, ((1, 4),)),
        "value_weight": centred(arg_keys[4], (D, ATT_HEADS * HEAD_DIM), D ** -0.5, 0.125, ((1, 4),)),
        "query_norm_gain": draw_query_norm_gain(jax.random.fold_in(arg_keys[18], 71), 0),
        "key_norm_gain": draw_key_norm_gain(jax.random.fold_in(arg_keys[18], 71), 0),
        "cumulative_gate": draw_cumulative_gate(jax.random.fold_in(arg_keys[18], 71), 0),
        "attention_norm_gain": jnp.clip(1.0 + 0.18 * jax.random.normal(arg_keys[8], (ATT_HEADS * HEAD_DIM,), jnp.float32), 0.1, 1.9),
        "recurrence_query_weight": centred(arg_keys[9], (D, RECURRENCE_HEADS * STATE_ROWS), D ** -0.5, 0.125, ((1, 4),)),
        "forget_weight": centred(arg_keys[10], (D, RECURRENCE_HEADS * STATE_ROWS), D ** -0.5, 0.125, ((1, 4),)),
        "recurrence_value_weight": centred(arg_keys[11], (D, RECURRENCE_HEADS * VAL_DIM), D ** -0.5, 0.125, ((1, 4),)),
        "output_gate_weight": centred(arg_keys[12], (D, RECURRENCE_HEADS * VAL_DIM), D ** -0.5, 0.125, ((1, 4),)),
        "gate_lower_slack": draw_gate_lower_slack(jax.random.fold_in(arg_keys[18], 71), 0),
        "extra_log_decay": draw_extra_log_decay(jax.random.fold_in(arg_keys[18], 71), 0),
        "recurrence_norm_gain": jnp.clip(1.0 + 0.18 * jax.random.normal(arg_keys[15], (RECURRENCE_HEADS * VAL_DIM,), jnp.float32), 0.1, 1.9),
        "attention_output_weight": centred(arg_keys[16], (ATT_HEADS * HEAD_DIM, D), (ATT_HEADS * HEAD_DIM + RECURRENCE_HEADS * VAL_DIM) ** -0.5, 0.125, ((0, 4),)),
        "recurrence_output_weight": centred(arg_keys[17], (RECURRENCE_HEADS * VAL_DIM, D), (ATT_HEADS * HEAD_DIM + RECURRENCE_HEADS * VAL_DIM) ** -0.5, 0.125, ((0, 4),)),
    }


EPSILON = 1e-06
HIGHEST_ACCURACY = lax.Precision.HIGHEST

def rms_rows(values, gain):
    squares = lax.optimization_barrier(jnp.mean(values * values, axis=-1, keepdims=True))
    return values * lax.rsqrt(squares + EPSILON) * gain

def recur_blocks(rec_query, forget_fraction, rec_value, decay_logarithm, states):
    length, head_number, keydim = rec_query.shape
    span_rows = BLOCK
    blocks = length // span_rows
    lower_tri = jnp.arange(span_rows)[:, None] >= jnp.arange(span_rows)[None, :]

    def to_blocks(values):
        return values.reshape(blocks, span_rows, head_number, values.shape[-1])

    def advance(carried, inputs):
        current_states, running = carried
        query_block, share_block, value_block, decay_blk = inputs
        within_block = jnp.cumsum(decay_blk, axis=0)
        differ = within_block[:, None] - within_block[None, :]
        fading = jnp.exp(jnp.where(lower_tri[:, :, None, None], differ, -jnp.inf))
        scores = jnp.einsum('thk,tshk,shk->tsh', query_block, fading, share_block, precision=HIGHEST_ACCURACY)
        inner_part = jnp.einsum('tsh,shv->thv', scores, value_block, precision=HIGHEST_ACCURACY)
        carried_piece = jnp.einsum('zbf,bfw->zbw', query_block * jnp.exp(within_block), current_states, precision=HIGHEST_ACCURACY)
        closing_state = within_block[-1]
        current_states = jnp.exp(closing_state)[:, :, None] * current_states + jnp.einsum('tfo,tfw->fow', share_block * jnp.exp(closing_state[None] - within_block), value_block, precision=HIGHEST_ACCURACY)
        visible_query = query_block * jnp.exp(running[None] + within_block)
        return ((current_states, running + closing_state), (inner_part + carried_piece, visible_query))
    zeros_run = jnp.zeros((head_number, keydim), jnp.float32)
    (states, running), (outputs, visible_query) = lax.scan(advance, (states, zeros_run), (to_blocks(rec_query), to_blocks(forget_fraction), to_blocks(rec_value), to_blocks(decay_logarithm)))
    return (outputs.reshape(length, head_number, -1), states, running, visible_query.reshape(length, head_number, keydim))

def attend_head(operands):
    head_query, head_key, head_value, head_cum = operands
    rows_blk = math.gcd(TOKEN_COUNT, 1024)
    score_scale = HEAD_DIM ** (-0.5)
    key_pos = jnp.arange(TOKEN_COUNT, dtype=jnp.int32)

    def one_block(block_index):
        first_row = (block_index * rows_blk).astype(jnp.int32)
        query_block = lax.dynamic_slice_in_dim(head_query, first_row, rows_blk, 0)
        cum_blk = lax.dynamic_slice_in_dim(head_cum, first_row, rows_blk, 0)
        scores = jnp.dot(query_block, head_key.T, preferred_element_type=jnp.float32) * score_scale
        scores = scores + cum_blk[:, None] - head_cum[None, :]
        query_pos = first_row + jnp.arange(rows_blk, dtype=jnp.int32)
        causal = key_pos[None, :] <= query_pos[:, None]
        scores = jnp.where(causal, scores, -jnp.inf)
        row_top = lax.optimization_barrier(jnp.max(scores, axis=-1))
        weights = jnp.exp(scores - row_top[:, None])
        totals = lax.optimization_barrier(jnp.sum(weights, axis=-1))
        summed = jnp.dot(weights.astype(jnp.bfloat16), head_value, preferred_element_type=jnp.float32)
        return (summed / totals[:, None], row_top + jnp.log(totals))
    outputs, log_sums = lax.map(one_block, jnp.arange(TOKEN_COUNT // rows_blk, dtype=jnp.int32))
    return (outputs.reshape(TOKEN_COUNT, HEAD_DIM), log_sums.reshape(TOKEN_COUNT))

def reference(layer_input_rows, input_norm_gain, query_weight, key_weight, value_weight, query_norm_gain, key_norm_gain, cumulative_gate, attention_norm_gain, recurrence_query_weight, forget_weight, recurrence_value_weight, output_gate_weight, gate_lower_slack, extra_log_decay, recurrence_norm_gain, attention_output_weight, recurrence_output_weight):
    normalized_input = rms_rows(layer_input_rows.astype(jnp.float32), input_norm_gain).astype(jnp.bfloat16)

    def project(weight):
        return jnp.dot(normalized_input, weight, preferred_element_type=jnp.float32)
    queries = rms_rows(project(query_weight).reshape(TOKEN_COUNT, ATT_HEADS, HEAD_DIM), query_norm_gain).astype(jnp.bfloat16)
    keys = rms_rows(project(key_weight).reshape(TOKEN_COUNT, ATT_HEADS, HEAD_DIM), key_norm_gain).astype(jnp.bfloat16)
    values = project(value_weight).astype(jnp.bfloat16).reshape(TOKEN_COUNT, ATT_HEADS, HEAD_DIM)
    attention, log_sum = lax.map(attend_head, (queries.transpose(1, 0, 2), keys.transpose(1, 0, 2), values.transpose(1, 0, 2), cumulative_gate.T))
    attn_out = rms_rows(attention.transpose(1, 0, 2), attention_norm_gain.reshape(ATT_HEADS, HEAD_DIM))
    attn_out = attn_out.astype(jnp.bfloat16).reshape(TOKEN_COUNT, ATT_HEADS * HEAD_DIM)
    rec_query = jax.nn.silu(project(recurrence_query_weight)).reshape(TOKEN_COUNT, RECURRENCE_HEADS, STATE_ROWS)
    forget_fraction = gate_lower_slack * jax.nn.sigmoid(-project(forget_weight))
    decay_logarithm = jnp.log1p(-forget_fraction).reshape(TOKEN_COUNT, RECURRENCE_HEADS, STATE_ROWS) + extra_log_decay[:, :, None]
    rec_value = lax.optimization_barrier(project(recurrence_value_weight).astype(jnp.bfloat16)).astype(jnp.float32)
    rec_value = rec_value.reshape(TOKEN_COUNT, RECURRENCE_HEADS, VAL_DIM)
    start_states = jnp.zeros((RECURRENCE_HEADS, STATE_ROWS, VAL_DIM), jnp.float32)
    recurrent_output = recur_blocks(rec_query, forget_fraction.reshape(TOKEN_COUNT, RECURRENCE_HEADS, STATE_ROWS), rec_value, decay_logarithm, start_states)[0]
    out_gate = jax.nn.silu(project(output_gate_weight)).reshape(TOKEN_COUNT, RECURRENCE_HEADS, VAL_DIM)
    rec_out = rms_rows(recurrent_output, recurrence_norm_gain.reshape(RECURRENCE_HEADS, VAL_DIM)) * out_gate
    rec_out = rec_out.astype(jnp.bfloat16).reshape(TOKEN_COUNT, RECURRENCE_HEADS * VAL_DIM)
    attn_cols = ATT_HEADS * HEAD_DIM // N_TP
    rec_cols = RECURRENCE_HEADS * VAL_DIM // N_TP

    def add_group(group_index, running_sum):
        first_attn = (group_index * attn_cols).astype(jnp.int32)
        first_rec = (group_index * rec_cols).astype(jnp.int32)
        attn_part = lax.dynamic_slice_in_dim(attn_out, first_attn, attn_cols, 1)
        attn_rows = lax.dynamic_slice_in_dim(attention_output_weight, first_attn, attn_cols, 0)
        rec_part = lax.dynamic_slice_in_dim(rec_out, first_rec, rec_cols, 1)
        rec_rows = lax.dynamic_slice_in_dim(recurrence_output_weight, first_rec, rec_cols, 0)
        partial_value = jnp.dot(attn_part, attn_rows, preferred_element_type=jnp.float32)
        partial_value = partial_value + jnp.dot(rec_part, rec_rows, preferred_element_type=jnp.float32)
        return running_sum + lax.optimization_barrier(partial_value.astype(jnp.bfloat16)).astype(jnp.float32)
    mixed_sum = lax.fori_loop(0, N_TP, add_group, jnp.zeros((TOKEN_COUNT, D), jnp.float32))
    return (mixed_sum.astype(jnp.bfloat16), log_sum.T)
```

```python
import functools
import math

import jax
import jax.numpy as jnp
from jax import lax
from jax.experimental import pallas as pl
from jax.experimental.pallas import tpu as pltpu
from jax.sharding import PartitionSpec as P

HEAD_DIM = 64
STATE_ROWS = 128
LANES = 128
EPSILON = 1e-06
MESH = pl.DeviceIdType.MESH
F32 = jnp.float32
BF16 = jnp.bfloat16


def dot(a, b):
    return jnp.dot(a, b, preferred_element_type=F32)


def parts_of(a, count):
    parts = []
    for _ in range(count):
        parts.append(a.astype(BF16))
        a = a - parts[-1].astype(F32)
    return parts


def dot_nt(a, b):
    return lax.dot_general(
        a, b, (((1,), (1,)), ((), ())), preferred_element_type=F32
    )


def iota(shape, axis):
    return lax.broadcasted_iota(jnp.int32, shape, axis)


def grid_of(count):
    columns = max(c for c in range(1, math.isqrt(count) + 1) if count % c == 0)
    return count // columns, columns


def kernel(
    sizes,
    x_hbm, wk_hbm, wv_hbm, wf_hbm, wrv_hbm, wrq_hbm, wq_hbm, wog_hbm, wao_hbm, wro_hbm,
    in_gain_hbm, q_gain_hbm, k_gain_hbm, gate_t_hbm, a_gain_hbm,
    slack_hbm, extra_t_hbm, r_gain_hbm,
    mixed_ref, logsum_ref,
    x_v, wkq_v, wvf_v, wrr_v, wog_v, wao_v, wro_v,
    xn, k_src, q_src, v_src, g_src, k_all, v_all, g_all, ga, q_in, s_buf, w_buf, m_s, l_s,
    o_src, lg_src, o_in, lg_in,
    inner, vq, og, ext, st, chain_in, chain_out, incoming, part, send2, recv1, recv2,
    in_gain, q_gain, k_gain, gate_t, a_gain, slack, extra_t, r_gain, rec_part,
    load_sem, k_send, v_send, q_send, g_send, k_recv, v_recv, q_recv, g_recv, k_fwd, v_fwd,
    o_send, o_recv, lg_send, lg_recv,
    st_send, st_recv, chain_send, chain_recv,
    s1_send, s1_recv, s2_send, s2_recv,
):
    nz, ny, ntp = sizes
    n_sp = nz * ny
    rows, width = x_v.shape
    cols = wog_v.shape[1]
    heads = cols // HEAD_DIM
    pairs = cols // LANES
    rec_heads = cols // STATE_ROWS
    chips = ntp // 2
    rb = rows // ntp
    half = rows // 2
    splits = s1_send.shape[1]
    part_cols = width // splits
    homes = n_sp // (2 * heads)
    members = 2 * homes

    sp, tp = lax.axis_index("sp"), lax.axis_index("tp")
    z, y = sp // ny, sp % ny
    chip, core = tp // 2, tp % 2
    partner = chip * 2 + (1 - core)

    group = sp // homes
    src_core, src_head = group % 2, group // 2
    primary = core == src_core
    member = (sp % homes) * 2 + core
    src_tp = chip * 2 + src_core

    def block_of(j):
        return j * members + (member if j % 2 == 0 else members - 1 - member)

    my_j = sp // members
    my_u = sp % members
    my_member = my_u + (my_j % 2) * (members - 1 - 2 * my_u)
    my_home, my_core = my_member // 2, my_member % 2

    def home_of(i, r):
        return (2 * i + core) * homes + r

    loads = []
    for i, (src, dst) in enumerate((
        (x_hbm, x_v), (wk_hbm, wkq_v.at[:, 0:cols]), (wq_hbm, wkq_v.at[:, cols : 2 * cols]),
        (wv_hbm, wvf_v.at[:, 0:cols]), (wf_hbm, wvf_v.at[:, cols : 2 * cols]),
        (wrv_hbm, wrr_v.at[:, 0:cols]), (wrq_hbm, wrr_v.at[:, cols : 2 * cols]),
        (wog_hbm, wog_v), (wao_hbm, wao_v), (wro_hbm, wro_v),
        (in_gain_hbm, in_gain), (q_gain_hbm, q_gain), (k_gain_hbm, k_gain),
        (gate_t_hbm, gate_t), (a_gain_hbm, a_gain), (slack_hbm, slack),
        (extra_t_hbm, extra_t), (r_gain_hbm, r_gain),
    )):
        loads.append(pltpu.make_async_copy(src, dst, load_sem.at[i]))

    for copy in loads[:1] + loads[10:] + loads[1:3]:
        copy.start()

    barrier = pltpu.get_barrier_semaphore()

    def greet(where):
        pl.semaphore_signal(barrier, inc=1, device_id=where, device_id_type=MESH)

    for k in range(n_sp):
        if k > 0:
            greet(((sp + k) % n_sp, tp))
        greet(((sp + k) % n_sp, partner))
    for k in range(1, chips):
        greet((sp, ((chip + k) % chips) * 2 + core))

    loads[0].wait()
    for copy in loads[10:]:
        copy.wait()
    for copy in loads[3:5]:
        copy.start()
    xf = x_v[...].astype(F32)
    scale = lax.rsqrt(jnp.mean(xf * xf, axis=-1, keepdims=True) + EPSILON)
    xn[...] = (xf * scale * in_gain[...]).astype(BF16)

    for i in range(heads):
        g_src[i] = gate_t[i : i + 1, :]

    block_ones = jnp.where(
        iota((cols, cols), 0) // HEAD_DIM == iota((cols, cols), 1) // HEAD_DIM, 1.0 / HEAD_DIM, 0.0
    ).astype(BF16)

    def head_norm(v, gain_ref):
        mean = sum(dot(p, block_ones) for p in parts_of(v * v, 2))
        gain = jnp.concatenate([gain_ref[...]] * heads, axis=1)
        return v * lax.rsqrt(mean + EPSILON) * gain

    loads[1].wait()
    loads[2].wait()
    for copy in loads[5:7]:
        copy.start()
    kq = dot(xn[...], wkq_v[...])
    keys = head_norm(kq[:, 0:cols], k_gain)
    first_half = iota((half, LANES), 1) < HEAD_DIM
    for p in range(pairs):
        low = keys[0:half, p * LANES : (p + 1) * LANES]
        high = keys[half:rows, p * LANES : (p + 1) * LANES]
        k_src[2 * p] = jnp.where(first_half, low, pltpu.roll(high, HEAD_DIM, 1)).astype(BF16)
        k_src[2 * p + 1] = jnp.where(first_half, pltpu.roll(low, HEAD_DIM, 1), high).astype(BF16)
    queries_t = (head_norm(kq[:, cols : 2 * cols], q_gain).astype(BF16).astype(F32)).T
    for i in range(heads):
        q_src[i] = (queries_t[i * HEAD_DIM : (i + 1) * HEAD_DIM, :] * HEAD_DIM ** (-0.5)).astype(BF16)

    greeted = 2 * n_sp - 1 + chips - 1
    pl.semaphore_wait(barrier, greeted)

    def remote(src, dst, send, recv, where):
        return pltpu.make_async_remote_copy(
            src_ref=src, dst_ref=dst, send_sem=send, recv_sem=recv,
            device_id=where, device_id_type=MESH,
        )

    def k_copy(i, r):
        return remote(
            k_src.at[i], k_all.at[sp], k_send.at[i, r], k_recv.at[sp], (home_of(i, r), tp)
        )

    def v_copy(i, r):
        return remote(
            v_src.at[i], v_all.at[sp], v_send.at[i, r], v_recv.at[sp], (home_of(i, r), tp)
        )

    def g_copy(i, r, c):
        return remote(
            g_src.at[i], g_all.at[sp], g_send.at[i, r, c], g_recv.at[sp],
            (home_of(i, r), tp if c == 0 else partner),
        )

    def q_copy(i):
        return remote(
            q_src.at[i], q_in.at[my_j], q_send.at[i], q_recv.at[my_j],
            (home_of(i, my_home), chip * 2 + my_core),
        )

    def spread(copies, local):
        for i in range(heads):
            for r in range(homes):
                @pl.when(home_of(i, r) != sp)
                def _():
                    copies(i, r).start()

                @pl.when(home_of(i, r) == sp)
                def _():
                    local(i)

    def keep_k(i):
        k_all[sp] = k_src[i]

    def keep_v(i):
        v_all[sp] = v_src[i]

    def keep_g(i):
        g_all[sp] = g_src[i]

    spread(k_copy, keep_k)
    for i in range(heads):
        stays = (home_of(i, my_home) == sp) & (my_core == core)

        @pl.when(jnp.logical_not(stays))
        def _():
            q_copy(i).start()

        @pl.when(stays)
        def _():
            q_in[my_j] = q_src[i]
    spread(lambda i, r: g_copy(i, r, 0), keep_g)
    for i in range(heads):
        for r in range(homes):
            g_copy(i, r, 1).start()

    loads[3].wait()
    loads[4].wait()
    for copy in loads[7:10]:
        copy.start()
    vf = dot(xn[...], wvf_v[...])
    values_t = vf[:, 0:cols].T.astype(BF16)
    for i in range(heads):
        v_src[i] = values_t[i * HEAD_DIM : (i + 1) * HEAD_DIM, :]
    spread(v_copy, keep_v)

    tri = iota((rows, rows), 0) >= iota((rows, rows), 1)
    tri_b = tri.astype(F32).astype(BF16)
    share = slack[...] / (1.0 + jnp.exp(vf[:, cols : 2 * cols]))
    run = sum(dot(tri_b, p) for p in parts_of(jnp.log1p(-share), 3))
    ext[...] = jnp.zeros_like(ext)
    ext[0:rec_heads, :] = extra_t[...]
    ext_row = sum(dot_nt(p, tri_b) for p in parts_of(ext[...], 3))
    ext_col = ext_row.T
    loads[5].wait()
    loads[6].wait()
    rr = dot(xn[...], wrr_v[...])
    rec_value = rr[:, 0:cols]
    rec_query = rr[:, cols : 2 * cols]
    rec_query = rec_query / (1.0 + jnp.exp(-rec_query))
    last = run[rows - 1 : rows]
    st_rows = STATE_ROWS + 16
    for j in range(rec_heads):
        lanes = slice(j * STATE_ROWS, (j + 1) * STATE_ROWS)
        e_col = ext_col[:, j : j + 1]
        e_row = ext_row[j : j + 1, :]
        e_last = e_row[:, rows - 1 : rows]
        left = share[:, lanes] * jnp.exp(last[:, lanes] - run[:, lanes] + (e_last - e_col))
        st[y, j * st_rows : j * st_rows + STATE_ROWS, :] = dot(
            rec_value[:, lanes].T.astype(BF16), left.astype(BF16)
        ).astype(BF16)
        st[y, j * st_rows + STATE_ROWS : (j + 1) * st_rows, :] = jnp.broadcast_to(
            jnp.exp(last[:, lanes] + e_last), (16, STATE_ROWS)
        ).astype(BF16)

    def st_copy(k):
        return remote(
            st.at[y], st.at[y], st_send.at[k], st_recv.at[y], (z * ny + (y + k) % ny, tp)
        )

    for k in range(1, ny):
        st_copy(k).start()

    grown = rec_query * jnp.exp(run)
    for j in range(rec_heads):
        lanes = slice(j * STATE_ROWS, (j + 1) * STATE_ROWS)
        e_col = ext_col[:, j : j + 1]
        e_row = ext_row[j : j + 1, :]
        value = rec_value[:, lanes].astype(BF16)
        scores = dot_nt(
            grown[:, lanes].astype(BF16), (share[:, lanes] * jnp.exp(-run[:, lanes])).astype(BF16)
        )
        fading = jnp.exp(jnp.where(tri, e_col - e_row, -jnp.inf))
        scores = jnp.where(tri, scores * fading, 0.0)
        inner[:, lanes] = dot(scores.astype(BF16), value)
        vq[:, lanes] = (grown[:, lanes] * jnp.exp(e_col)).astype(BF16)

    chain_copy = remote(
        chain_out, chain_in, chain_send, chain_recv, ((sp + ny) % n_sp, tp)
    )

    for k in range(1, ny):
        other = (y + k) % ny
        remote(
            st.at[other], st.at[other], st_send.at[0], st_recv.at[other], (sp, partner)
        ).wait_recv()

    def advance_chain():
        for j in range(rec_heads):
            rows_at = slice(j * STATE_ROWS, (j + 1) * STATE_ROWS)
            state = chain_in[rows_at, :].astype(F32)
            for k in range(ny):
                @pl.when(y == k)
                def _():
                    incoming[rows_at, :] = state.astype(BF16)

                base = j * st_rows
                decay = st[k, base + STATE_ROWS : base + st_rows, :].astype(F32)[0:1]
                state = state * decay + st[k, base : base + STATE_ROWS, :].astype(F32)
            chain_out[rows_at, :] = state.astype(BF16)

        @pl.when(z < nz - 1)
        def _():
            chain_copy.start()

    @pl.when(z == 0)
    def _():
        chain_in[...] = jnp.zeros_like(chain_in)
        advance_chain()

    def chain_at(here):
        @pl.when(here)
        def _():
            chain_copy.wait_recv()
            advance_chain()

    loads[7].wait()
    gate_out = dot(xn[...], wog_v[...])
    og[...] = gate_out / (1.0 + jnp.exp(-gate_out))

    for t in range(n_sp):
        @pl.when((sp != t) | jnp.logical_not(primary))
        def _():
            remote(
                g_all.at[t], g_all.at[t], g_send.at[0, 0, 0], g_recv.at[t], (sp, partner)
            ).wait_recv()

    gate_cols = jnp.concatenate(
        [g_all[t, :, h * half : (h + 1) * half] for t in range(n_sp) for h in range(2)], axis=0
    ).T
    gate_parts = jnp.concatenate(
        [p.astype(F32) for p in parts_of(gate_cols, 3)]
        + [jnp.zeros((half, LANES - 6 * n_sp), F32)] * (6 * n_sp < LANES), axis=1
    )
    lane_block = (iota((half, LANES), 1) % (2 * n_sp)) // 2
    for t in range(n_sp):
        ga[t] = jnp.where(lane_block == t, gate_parts, 0.0).astype(BF16)

    def wait_all(ref, fwd, recv):
        for t in range(n_sp):
            copy = remote(ref.at[t], ref.at[t], fwd.at[t], recv.at[t], (sp, partner))

            @pl.when((sp != t) | jnp.logical_not(primary))
            def _():
                copy.wait_recv()

            @pl.when(primary)
            def _():
                copy.start()

    chain_at(z == 1)
    wait_all(k_all, k_fwd, k_recv)
    chain_at(z == 2)

    minus = jnp.where(
        iota((LANES, 2 * rows), 0) % 2 == iota((LANES, 2 * rows), 1) // rows, -1.0, 0.0
    ).astype(BF16)
    ahead = (
        iota((half, 2 * rows), 0) + half * (iota((half, 2 * rows), 1) // rows)
        - iota((half, 2 * rows), 1) % rows
    )
    first = [members * j * (j + 1) // 2 for j in range(heads)]

    def weigh(j):
        remote(
            q_in.at[j], q_in.at[j], q_send.at[0], q_recv.at[j], (sp, partner)
        )
        kept = (block_of(j) == sp) & primary

        @pl.when(jnp.logical_not(kept))
        def _():
            remote(
                q_in.at[j], q_in.at[j], q_send.at[0], q_recv.at[j], (sp, partner)
            ).wait_recv()

        q = q_in[j]
        none = jnp.zeros_like(q)
        right = jnp.concatenate(
            [jnp.concatenate([q, none], axis=1), jnp.concatenate([none, q], axis=1), minus], axis=0
        )
        top = None
        for t in range((j + 1) * members):
            s = dot(jnp.concatenate([k_all[t], ga[t]], axis=1), right)
            if t >= j * members:
                s = jnp.where(ahead <= (block_of(j) - t) * rows, s, -jnp.inf)
            s_buf[t] = s
            here = jnp.max(s, axis=0, keepdims=True)
            top = here if top is None else jnp.maximum(top, here)
        top = jnp.maximum(top[:, 0:rows], top[:, rows : 2 * rows])
        m_s[j] = top
        top = jnp.concatenate([top, top], axis=1)
        total = None
        for t in range((j + 1) * members):
            w = jnp.exp(s_buf[t] - top)
            here = jnp.sum(w, axis=0, keepdims=True)
            total = here if total is None else total + here
            w = w.astype(BF16)
            w_buf[first[j] + t, 0:half, :] = w[:, 0:rows]
            w_buf[first[j] + t, half:rows, :] = w[:, rows : 2 * rows]
        l_s[j] = total[:, 0:rows] + total[:, rows : 2 * rows]

    def o_copy(j):
        return remote(
            o_src.at[j], o_in.at[src_head], o_send.at[j], o_recv.at[src_head],
            (block_of(j), src_tp),
        )

    def lg_copy(j):
        return remote(
            lg_src.at[j], lg_in.at[src_head], lg_send.at[j], lg_recv.at[src_head],
            (block_of(j), src_tp),
        )

    def finish(j):
        n = (j + 1) * members
        summed = [
            sum(dot(v_all[t], w_buf[first[j] + t]) for t in range(u, n, 2)) for u in range(2)
        ]
        out = (summed[0] + summed[1]) / l_s[j]
        mean = jnp.mean(out * out, axis=0, keepdims=True)
        o_src[j] = (out * lax.rsqrt(mean + EPSILON)).astype(BF16)
        lg_src[j] = m_s[j] + jnp.log(l_s[j])
        kept = (block_of(j) == sp) & primary

        @pl.when(jnp.logical_not(kept))
        def _():
            o_copy(j).start()
            lg_copy(j).start()

        @pl.when(kept)
        def _():
            o_in[src_head] = o_src[j]
            lg_in[src_head] = lg_src[j]

    for j in range(heads):
        weigh(j)
    wait_all(v_all, v_fwd, v_recv)
    for j in range(heads):
        finish(j)

    chain_at(z >= 3)
    for j in range(rec_heads):
        lanes = slice(j * STATE_ROWS, (j + 1) * STATE_ROWS)
        out = inner[:, lanes] + dot_nt(vq[:, lanes], incoming[lanes, :])
        mean = jnp.mean(out * out, axis=-1, keepdims=True)
        out = out * lax.rsqrt(mean + EPSILON) * r_gain[:, lanes] * og[:, lanes]
        vq[:, lanes] = out.astype(BF16)
    loads[9].wait()
    rec_part[...] = dot(vq[...], wro_v[...])
    loads[8].wait()

    for i in range(heads):
        kept = (home_of(i, my_home) == sp) & (my_core == core)

        @pl.when(jnp.logical_not(kept))
        def _():
            remote(
                o_in.at[i], o_in.at[i], o_send.at[0], o_recv.at[i], (sp, partner)
            ).wait_recv()
            remote(
                lg_in.at[i], lg_in.at[i], lg_send.at[0], lg_recv.at[i], (sp, partner)
            ).wait_recv()

    for i in range(heads):
        logsum_ref[i : i + 1, :] = lg_in[i] + gate_t[i : i + 1, :]
    attn_t = jnp.concatenate([o_in[i].astype(F32) for i in range(heads)], axis=0)
    attn_out = (attn_t.T * a_gain[...]).astype(BF16)

    def rows_of(which_chip, which_core):
        return pl.ds(pl.multiple_of((which_chip * 2 + which_core) * rb, rb), rb)

    def columns(q):
        return slice(q * part_cols, (q + 1) * part_cols)

    def within(j, q):
        return pltpu.make_async_remote_copy(
            src_ref=part.at[q, rows_of(j, 1 - core)], dst_ref=recv1.at[j, q],
            send_sem=s1_send.at[j, q], recv_sem=s1_recv.at[j, q], device_id=(sp, partner),
            device_id_type=MESH,
        )

    def between(j, q):
        return pltpu.make_async_remote_copy(
            src_ref=send2.at[j, q], dst_ref=recv2.at[chip, q], send_sem=s2_send.at[j, q],
            recv_sem=s2_recv.at[chip, q], device_id=(sp, j * 2 + core), device_id_type=MESH,
        )

    order = [(chip + k) % chips for k in range(1, chips)]

    def chip_sum(j, q):
        within(j, q).wait_recv()
        return part[q, rows_of(j, core), :].astype(F32) + recv1[j, q].astype(F32)

    def send_sums(q):
        for j in order:
            send2[j, q] = chip_sum(j, q).astype(BF16)
            between(j, q).start()

    for q in range(splits):
        part[q] = (
            dot(attn_out, wao_v[:, columns(q)]) + rec_part[:, columns(q)]
        ).astype(BF16)
        for j in order:
            within(j, q).start()
        if q > 0:
            send_sums(q - 1)
    send_sums(splits - 1)
    for q in range(splits):
        within(chip, q).start()
    for q in range(splits):
        total = chip_sum(chip, q)
        for j in order:
            pltpu.make_async_remote_copy(
                src_ref=send2.at[j, q], dst_ref=recv2.at[j, q], send_sem=s2_send.at[j, q],
                recv_sem=s2_recv.at[j, q], device_id=(sp, partner), device_id_type=MESH,
            ).wait_recv()
            total = total + recv2[j, q].astype(F32)
        mixed_ref[:, columns(q)] = total.astype(BF16)

    for q in range(splits):
        for j in order + [chip]:
            within(j, q).wait_send()
        for j in order:
            between(j, q).wait_send()
    for k in range(1, ny):
        st_copy(k).wait_send()

    @pl.when(z < nz - 1)
    def _():
        chain_copy.wait_send()

    for i in range(heads):
        for r in range(homes):
            @pl.when(home_of(i, r) != sp)
            def _():
                k_copy(i, r).wait_send()
                v_copy(i, r).wait_send()
                g_copy(i, r, 0).wait_send()

            g_copy(i, r, 1).wait_send()

        @pl.when((home_of(i, my_home) != sp) | (my_core != core))
        def _():
            q_copy(i).wait_send()

    @pl.when(primary)
    def _():
        for t in range(n_sp):
            remote(k_all.at[t], k_all.at[t], k_fwd.at[t], k_recv.at[t], (sp, partner)).wait_send()
            remote(v_all.at[t], v_all.at[t], v_fwd.at[t], v_recv.at[t], (sp, partner)).wait_send()

    for j in range(heads):
        @pl.when((block_of(j) != sp) | jnp.logical_not(primary))
        def _():
            o_copy(j).wait_send()
            lg_copy(j).wait_send()


def body(
    n_sp, n_tp,
    layer_input_rows, input_norm_gain, query_weight, key_weight, value_weight, query_norm_gain,
    key_norm_gain, cumulative_gate, attention_norm_gain, recurrence_query_weight, forget_weight,
    recurrence_value_weight, output_gate_weight, gate_lower_slack, extra_log_decay,
    recurrence_norm_gain, attention_output_weight, recurrence_output_weight,
):
    nz, ny = grid_of(n_sp)
    rows, width = layer_input_rows.shape
    cols = query_weight.shape[1]
    heads, pairs, rec_heads = cols // HEAD_DIM, cols // LANES, cols // STATE_ROWS
    rb, chips = rows // n_tp, n_tp // 2
    half = rows // 2
    homes = n_sp // (2 * heads)
    blocks = 2 * homes * heads * (heads + 1) // 2
    splits = math.gcd(width // LANES, 4)
    weight = pltpu.VMEM((width, cols), BF16)
    two_weights = pltpu.VMEM((width, 2 * cols), BF16)
    out_weight = pltpu.VMEM((cols, width), BF16)
    dma = pltpu.SemaphoreType.DMA
    any_space = pl.BlockSpec(memory_space=pl.ANY)
    vmem = pl.BlockSpec(memory_space=pltpu.VMEM)
    mixed, log_sum = pl.pallas_call(
        functools.partial(kernel, (nz, ny, n_tp)),
        name="mixer",
        out_shape=(
            jax.ShapeDtypeStruct((rb, width), BF16),
            jax.ShapeDtypeStruct((heads, rows), F32),
        ),
        in_specs=[any_space] * 18,
        out_specs=(vmem, vmem),
        scratch_shapes=[
            pltpu.VMEM((rows, width), BF16),
            *([two_weights] * 3), weight, out_weight, out_weight,
            pltpu.VMEM((rows, width), BF16),
            pltpu.VMEM((heads, half, LANES), BF16),
            pltpu.VMEM((heads, HEAD_DIM, rows), BF16),
            pltpu.VMEM((heads, HEAD_DIM, rows), BF16),
            pltpu.VMEM((heads, 1, rows), F32),
            pltpu.VMEM((n_sp, half, LANES), BF16),
            pltpu.VMEM((n_sp, HEAD_DIM, rows), BF16),
            pltpu.VMEM((n_sp, 1, rows), F32),
            pltpu.VMEM((n_sp, half, LANES), BF16),
            pltpu.VMEM((heads, HEAD_DIM, rows), BF16),
            pltpu.VMEM((n_sp, half, 2 * rows), F32),
            pltpu.VMEM((blocks, rows, rows), BF16),
            pltpu.VMEM((heads, 1, rows), F32),
            pltpu.VMEM((heads, 1, rows), F32),
            pltpu.VMEM((heads, HEAD_DIM, rows), BF16),
            pltpu.VMEM((heads, 1, rows), F32),
            pltpu.VMEM((heads, HEAD_DIM, rows), BF16),
            pltpu.VMEM((heads, 1, rows), F32),
            pltpu.VMEM((rows, cols), F32),
            pltpu.VMEM((rows, cols), BF16),
            pltpu.VMEM((rows, cols), F32),
            pltpu.VMEM((8, rows), F32),
            pltpu.VMEM((ny, rec_heads * (STATE_ROWS + 16), STATE_ROWS), BF16),
            pltpu.VMEM((cols, STATE_ROWS), BF16),
            pltpu.VMEM((cols, STATE_ROWS), BF16),
            pltpu.VMEM((cols, STATE_ROWS), BF16),
            pltpu.VMEM((splits, rows, width // splits), BF16),
            *([pltpu.VMEM((chips, splits, rb, width // splits), BF16)] * 3),
            *([pltpu.VMEM((1, n), F32) for n in (width, HEAD_DIM, HEAD_DIM)]),
            pltpu.VMEM((heads, rows), F32),
            pltpu.VMEM((1, cols), F32),
            pltpu.VMEM((1, cols), F32),
            pltpu.VMEM((rec_heads, rows), F32),
            pltpu.VMEM((1, cols), F32),
            pltpu.VMEM((rows, width), F32),
            dma((18,)),
            dma((heads, homes)), dma((heads, homes)), dma((heads,)), dma((heads, homes, 2)),
            dma((n_sp,)), dma((n_sp,)), dma((heads,)), dma((n_sp,)), dma((n_sp,)), dma((n_sp,)),
            *([dma((heads,))] * 4),
            dma((ny,)), dma((ny,)), dma, dma,
            *([dma((chips, splits))] * 4),
        ],
        compiler_params=pltpu.CompilerParams(
            collective_id=0, has_side_effects=True, vmem_limit_bytes=60 * 1024 * 1024
        ),
    )(
        layer_input_rows, key_weight, value_weight, forget_weight, recurrence_value_weight,
        recurrence_query_weight, query_weight, output_gate_weight, attention_output_weight,
        recurrence_output_weight,
        input_norm_gain.reshape(1, -1), query_norm_gain.reshape(1, -1),
        key_norm_gain.reshape(1, -1), cumulative_gate.T, attention_norm_gain.reshape(1, -1),
        gate_lower_slack.reshape(1, -1), extra_log_decay.T, recurrence_norm_gain.reshape(1, -1),
    )
    return mixed, log_sum.T


def solution(mesh):
    return jax.shard_map(
        functools.partial(body, mesh.shape["sp"], mesh.shape["tp"]),
        mesh=mesh,
        in_specs=(
            P("sp", None),
            P(),
            P(None, "tp"),
            P(None, "tp"),
            P(None, "tp"),
            P(),
            P(),
            P("sp", "tp"),
            P("tp"),
            P(None, "tp"),
            P(None, "tp"),
            P(None, "tp"),
            P(None, "tp"),
            P("tp"),
            P("sp", "tp"),
            P("tp"),
            P("tp", None),
            P("tp", None),
        ),
        out_specs=(P(("sp", "tp"), None), P("sp", "tp")),
        check_vma=False,
    )
```

```python
import functools
import math

import jax
import jax.numpy as jnp
from jax import lax
from jax.experimental import pallas as pl
from jax.experimental.pallas import tpu as pltpu
from jax.sharding import PartitionSpec as P

HEAD_DIM = 64
STATE_ROWS = 128
LANES = 128
EPSILON = 1e-06
MESH = pl.DeviceIdType.MESH
F32 = jnp.float32
BF16 = jnp.bfloat16


def dot(a, b):
    return jnp.dot(a, b, preferred_element_type=F32)


def parts_of(a, count):
    parts = []
    for _ in range(count):
        parts.append(a.astype(BF16))
        a = a - parts[-1].astype(F32)
    return parts


def dot_nt(a, b):
    return lax.dot_general(
        a, b, (((1,), (1,)), ((), ())), preferred_element_type=F32
    )


def iota(shape, axis):
    return lax.broadcasted_iota(jnp.int32, shape, axis)


def grid_of(count):
    columns = max(c for c in range(1, math.isqrt(count) + 1) if count % c == 0)
    return count // columns, columns


def kernel(
    sizes,
    x_hbm, wk_hbm, wv_hbm, wf_hbm, wrv_hbm, wrq_hbm, wq_hbm, wog_hbm, wao_hbm, wro_hbm,
    in_gain_hbm, q_gain_hbm, k_gain_hbm, gate_t_hbm, a_gain_hbm,
    slack_hbm, extra_t_hbm, r_gain_hbm,
    mixed_ref, logsum_ref,
    x_v, wkq_v, wfr_v, wvr_v, wog_v, wao_v, wro_v,
    xn, k_src, q_src, v_src, g_src, k_all, v_all, g_all, ga, q_in, s_buf, w_buf, m_s, l_s,
    o_src, lg_src, o_in, lg_in,
    inner, vq, og, ext, st, chain_in, chain_out, incoming, part, send2, recv1, recv2,
    in_gain, q_gain, k_gain, gate_t, a_gain, slack, extra_t, r_gain, rec_part,
    load_sem, k_send, v_send, q_send, g_send, k_recv, v_recv, q_recv, g_recv, k_fwd, v_fwd,
    o_send, o_recv, lg_send, lg_recv,
    st_send, st_recv, chain_send, chain_recv,
    s1_send, s1_recv, s2_send, s2_recv,
):
    nz, ny, ntp = sizes
    n_sp = nz * ny
    rows, width = x_v.shape
    cols = wog_v.shape[1]
    heads = cols // HEAD_DIM
    pairs = cols // LANES
    rec_heads = cols // STATE_ROWS
    chips = ntp // 2
    rb = rows // ntp
    half = rows // 2
    splits = s1_send.shape[1]
    part_cols = width // splits
    homes = n_sp // (2 * heads)
    members = 2 * homes

    sp, tp = lax.axis_index("sp"), lax.axis_index("tp")
    z, y = sp // ny, sp % ny
    chip, core = tp // 2, tp % 2
    partner = chip * 2 + (1 - core)

    group = sp // homes
    src_core, src_head = group % 2, group // 2
    primary = core == src_core
    member = (sp % homes) * 2 + core
    src_tp = chip * 2 + src_core

    def block_of(j):
        return j * members + (member if j % 2 == 0 else members - 1 - member)

    my_j = sp // members
    my_u = sp % members
    my_member = my_u + (my_j % 2) * (members - 1 - 2 * my_u)
    my_home, my_core = my_member // 2, my_member % 2

    def home_of(i, r):
        return (2 * i + core) * homes + r

    loads = []
    for i, (src, dst) in enumerate((
        (x_hbm, x_v), (wk_hbm, wkq_v.at[:, 0:cols]), (wq_hbm, wkq_v.at[:, cols : 2 * cols]),
        (wf_hbm, wfr_v.at[:, 0:cols]), (wrv_hbm, wfr_v.at[:, cols : 2 * cols]),
        (wv_hbm, wvr_v.at[:, 0:cols]), (wrq_hbm, wvr_v.at[:, cols : 2 * cols]),
        (wog_hbm, wog_v), (wao_hbm, wao_v), (wro_hbm, wro_v),
        (in_gain_hbm, in_gain), (q_gain_hbm, q_gain), (k_gain_hbm, k_gain),
        (gate_t_hbm, gate_t), (a_gain_hbm, a_gain), (slack_hbm, slack),
        (extra_t_hbm, extra_t), (r_gain_hbm, r_gain),
    )):
        loads.append(pltpu.make_async_copy(src, dst, load_sem.at[i]))

    for copy in loads[:1] + loads[10:] + loads[1:3]:
        copy.start()

    barrier = pltpu.get_barrier_semaphore()

    def greet(where):
        pl.semaphore_signal(barrier, inc=1, device_id=where, device_id_type=MESH)

    for k in range(n_sp):
        if k > 0:
            greet(((sp + k) % n_sp, tp))
        greet(((sp + k) % n_sp, partner))
    for k in range(1, chips):
        greet((sp, ((chip + k) % chips) * 2 + core))

    loads[0].wait()
    for copy in loads[10:]:
        copy.wait()
    for copy in loads[3:5]:
        copy.start()
    xf = x_v[...].astype(F32)
    scale = lax.rsqrt(jnp.mean(xf * xf, axis=-1, keepdims=True) + EPSILON)
    xn[...] = (xf * scale * in_gain[...]).astype(BF16)

    for i in range(heads):
        g_src[i] = gate_t[i : i + 1, :]

    block_ones = jnp.where(
        iota((cols, cols), 0) // HEAD_DIM == iota((cols, cols), 1) // HEAD_DIM, 1.0 / HEAD_DIM, 0.0
    ).astype(BF16)

    def head_norm(v, gain_ref):
        mean = sum(dot(p, block_ones) for p in parts_of(v * v, 2))
        gain = jnp.concatenate([gain_ref[...]] * heads, axis=1)
        return v * lax.rsqrt(mean + EPSILON) * gain

    loads[1].wait()
    loads[2].wait()
    for copy in loads[5:7]:
        copy.start()
    kq = dot(xn[...], wkq_v[...])
    keys = head_norm(kq[:, 0:cols], k_gain)
    first_half = iota((half, LANES), 1) < HEAD_DIM
    for p in range(pairs):
        low = keys[0:half, p * LANES : (p + 1) * LANES]
        high = keys[half:rows, p * LANES : (p + 1) * LANES]
        k_src[2 * p] = jnp.where(first_half, low, pltpu.roll(high, HEAD_DIM, 1)).astype(BF16)
        k_src[2 * p + 1] = jnp.where(first_half, pltpu.roll(low, HEAD_DIM, 1), high).astype(BF16)
    queries_t = (head_norm(kq[:, cols : 2 * cols], q_gain).astype(BF16).astype(F32)).T
    for i in range(heads):
        q_src[i] = (queries_t[i * HEAD_DIM : (i + 1) * HEAD_DIM, :] * HEAD_DIM ** (-0.5)).astype(BF16)

    def remote(src, dst, send, recv, where):
        return pltpu.make_async_remote_copy(
            src_ref=src, dst_ref=dst, send_sem=send, recv_sem=recv,
            device_id=where, device_id_type=MESH,
        )

    def k_copy(i, r):
        return remote(
            k_src.at[i], k_all.at[sp], k_send.at[i, r], k_recv.at[sp], (home_of(i, r), tp)
        )

    def v_copy(i, r):
        return remote(
            v_src.at[i], v_all.at[sp], v_send.at[i, r], v_recv.at[sp], (home_of(i, r), tp)
        )

    def g_copy(i, r, c):
        return remote(
            g_src.at[i], g_all.at[sp], g_send.at[i, r, c], g_recv.at[sp],
            (home_of(i, r), tp if c == 0 else partner),
        )

    def q_copy(i):
        return remote(
            q_src.at[i], q_in.at[my_j], q_send.at[i], q_recv.at[my_j],
            (home_of(i, my_home), chip * 2 + my_core),
        )

    turns = [(src_head + k) % heads for k in range(heads)]

    def spread(copies, local):
        for i in turns:
            for r in range(homes):
                @pl.when(home_of(i, r) != sp)
                def _():
                    copies(i, r).start()

                @pl.when(home_of(i, r) == sp)
                def _():
                    local(i)

    def keep_k(i):
        k_all[sp] = k_src[i]

    def keep_v(i):
        v_all[sp] = v_src[i]

    def keep_g(i):
        g_all[sp] = g_src[i]

    def begin():
        pl.semaphore_wait(barrier, 2 * n_sp - 1 + chips - 1)

    def send_keys_and_queries():
        spread(lambda i, r: g_copy(i, r, 0), keep_g)
        for i in range(heads):
            for r in range(homes):
                g_copy(i, r, 1).start()
        spread(k_copy, keep_k)
        for i in turns:
            stays = (home_of(i, my_home) == sp) & (my_core == core)

            @pl.when(jnp.logical_not(stays))
            def _():
                q_copy(i).start()

            @pl.when(stays)
            def _():
                q_in[my_j] = q_src[i]

    early = z == 0

    @pl.when(jnp.logical_not(early))
    def _():
        begin()
        send_keys_and_queries()

    tri = iota((rows, rows), 0) >= iota((rows, rows), 1)
    tri_b = tri.astype(F32).astype(BF16)
    loads[3].wait()
    loads[4].wait()
    for copy in loads[7:10]:
        copy.start()
    fr = dot(xn[...], wfr_v[...])
    share = slack[...] / (1.0 + jnp.exp(fr[:, 0:cols]))
    rec_value = fr[:, cols : 2 * cols]
    run = sum(dot(tri_b, p) for p in parts_of(jnp.log1p(-share), 3))
    ext[...] = jnp.zeros_like(ext)
    ext[0:rec_heads, :] = extra_t[...]
    ext_row = sum(dot_nt(p, tri_b) for p in parts_of(ext[...], 3))
    ext_col = ext_row.T
    last = run[rows - 1 : rows]
    st_rows = STATE_ROWS + 16
    for j in range(rec_heads):
        lanes = slice(j * STATE_ROWS, (j + 1) * STATE_ROWS)
        e_col = ext_col[:, j : j + 1]
        e_row = ext_row[j : j + 1, :]
        e_last = e_row[:, rows - 1 : rows]
        left = share[:, lanes] * jnp.exp(last[:, lanes] - run[:, lanes] + (e_last - e_col))
        st[y, j * st_rows : j * st_rows + STATE_ROWS, :] = dot(
            rec_value[:, lanes].T.astype(BF16), left.astype(BF16)
        ).astype(BF16)
        st[y, j * st_rows + STATE_ROWS : (j + 1) * st_rows, :] = jnp.broadcast_to(
            jnp.exp(last[:, lanes] + e_last), (16, STATE_ROWS)
        ).astype(BF16)

    def st_copy(k):
        return remote(
            st.at[y], st.at[y], st_send.at[k], st_recv.at[y], (z * ny + (y + k) % ny, tp)
        )

    @pl.when(early)
    def _():
        begin()

    for k in range(1, ny):
        st_copy(k).start()

    @pl.when(early)
    def _():
        send_keys_and_queries()

    loads[5].wait()
    loads[6].wait()
    vr = dot(xn[...], wvr_v[...])
    values_t = vr[:, 0:cols].T.astype(BF16)
    for i in range(heads):
        v_src[i] = values_t[i * HEAD_DIM : (i + 1) * HEAD_DIM, :]
    spread(v_copy, keep_v)

    rec_query = vr[:, cols : 2 * cols]
    rec_query = rec_query / (1.0 + jnp.exp(-rec_query))
    grown = rec_query * jnp.exp(run)
    for j in range(rec_heads):
        lanes = slice(j * STATE_ROWS, (j + 1) * STATE_ROWS)
        e_col = ext_col[:, j : j + 1]
        e_row = ext_row[j : j + 1, :]
        value = rec_value[:, lanes].astype(BF16)
        scores = dot_nt(
            grown[:, lanes].astype(BF16), (share[:, lanes] * jnp.exp(-run[:, lanes])).astype(BF16)
        )
        fading = jnp.exp(jnp.where(tri, e_col - e_row, -jnp.inf))
        scores = jnp.where(tri, scores * fading, 0.0)
        inner[:, lanes] = dot(scores.astype(BF16), value)
        vq[:, lanes] = (grown[:, lanes] * jnp.exp(e_col)).astype(BF16)

    loads[7].wait()
    gate_out = dot(xn[...], wog_v[...])
    og[...] = gate_out / (1.0 + jnp.exp(-gate_out))

    for k in range(1, ny):
        other = (y + k) % ny
        remote(
            st.at[other], st.at[other], st_send.at[0], st_recv.at[other], (sp, partner)
        ).wait_recv()

    def chain_copy(j):
        return remote(
            chain_out.at[j], chain_in.at[j], chain_send.at[j], chain_recv.at[j],
            ((sp + ny) % n_sp, tp),
        )

    def advance_chain(received):
        for j in range(rec_heads):
            if received:
                chain_copy(j).wait_recv()
                state = chain_in[j].astype(F32)
            else:
                state = jnp.zeros((STATE_ROWS, STATE_ROWS), F32)
            for k in range(ny):
                @pl.when(y == k)
                def _():
                    incoming[j] = state.astype(BF16)

                base = j * st_rows
                decay = st[k, base + STATE_ROWS : base + st_rows, :].astype(F32)[0:1]
                state = state * decay + st[k, base : base + STATE_ROWS, :].astype(F32)
            chain_out[j] = state.astype(BF16)

            @pl.when(z < nz - 1)
            def _():
                chain_copy(j).start()

    @pl.when(z == 0)
    def _():
        advance_chain(False)

    def chain_at(here):
        @pl.when(here)
        def _():
            advance_chain(True)

    for t in range(n_sp):
        @pl.when((sp != t) | jnp.logical_not(primary))
        def _():
            remote(
                g_all.at[t], g_all.at[t], g_send.at[0, 0, 0], g_recv.at[t], (sp, partner)
            ).wait_recv()

    gate_cols = jnp.concatenate(
        [g_all[t, :, h * half : (h + 1) * half] for t in range(n_sp) for h in range(2)], axis=0
    ).T
    gate_parts = jnp.concatenate(
        [p.astype(F32) for p in parts_of(gate_cols, 3)]
        + [jnp.zeros((half, LANES - 6 * n_sp), F32)] * (6 * n_sp < LANES), axis=1
    )
    lane_block = (iota((half, LANES), 1) % (2 * n_sp)) // 2
    for t in range(n_sp):
        ga[t] = jnp.where(lane_block == t, gate_parts, 0.0).astype(BF16)

    def take(ref, fwd, recv, j):
        for t in range(j * members, (j + 1) * members):
            copy = remote(ref.at[t], ref.at[t], fwd.at[t], recv.at[t], (sp, partner))

            @pl.when((sp != t) | jnp.logical_not(primary))
            def _():
                copy.wait_recv()

            @pl.when(primary)
            def _():
                copy.start()

    def take_keys(j):
        take(k_all, k_fwd, k_recv, j)

    def take_values(j):
        take(v_all, v_fwd, v_recv, j)

    minus = jnp.where(
        iota((LANES, 2 * rows), 0) % 2 == iota((LANES, 2 * rows), 1) // rows, -1.0, 0.0
    ).astype(BF16)
    ahead = (
        iota((half, 2 * rows), 0) + half * (iota((half, 2 * rows), 1) // rows)
        - iota((half, 2 * rows), 1) % rows
    )
    first = [members * j * (j + 1) // 2 for j in range(heads)]

    def weigh(j):
        remote(
            q_in.at[j], q_in.at[j], q_send.at[0], q_recv.at[j], (sp, partner)
        )
        kept = (block_of(j) == sp) & primary

        @pl.when(jnp.logical_not(kept))
        def _():
            remote(
                q_in.at[j], q_in.at[j], q_send.at[0], q_recv.at[j], (sp, partner)
            ).wait_recv()

        q = q_in[j]
        none = jnp.zeros_like(q)
        right = jnp.concatenate(
            [jnp.concatenate([q, none], axis=1), jnp.concatenate([none, q], axis=1), minus], axis=0
        )
        top = None
        for t in range((j + 1) * members):
            s = dot(jnp.concatenate([k_all[t], ga[t]], axis=1), right)
            if t >= j * members:
                s = jnp.where(ahead <= (block_of(j) - t) * rows, s, -jnp.inf)
            s_buf[t] = s
            here = jnp.max(s, axis=0, keepdims=True)
            top = here if top is None else jnp.maximum(top, here)
        top = jnp.maximum(top[:, 0:rows], top[:, rows : 2 * rows])
        m_s[j] = top
        top = jnp.concatenate([top, top], axis=1)
        total = None
        for t in range((j + 1) * members):
            w = jnp.exp(s_buf[t] - top)
            here = jnp.sum(w, axis=0, keepdims=True)
            total = here if total is None else total + here
            w = w.astype(BF16)
            w_buf[first[j] + t, 0:half, :] = w[:, 0:rows]
            w_buf[first[j] + t, half:rows, :] = w[:, rows : 2 * rows]
        l_s[j] = total[:, 0:rows] + total[:, rows : 2 * rows]

    def o_copy(j):
        return remote(
            o_src.at[j], o_in.at[src_head], o_send.at[j], o_recv.at[src_head],
            (block_of(j), src_tp),
        )

    def lg_copy(j):
        return remote(
            lg_src.at[j], lg_in.at[src_head], lg_send.at[j], lg_recv.at[src_head],
            (block_of(j), src_tp),
        )

    def finish(j):
        n = (j + 1) * members
        summed = [
            sum(dot(v_all[t], w_buf[first[j] + t]) for t in range(u, n, 2)) for u in range(2)
        ]
        out = (summed[0] + summed[1]) / l_s[j]
        mean = jnp.mean(out * out, axis=0, keepdims=True)
        o_src[j] = (out * lax.rsqrt(mean + EPSILON)).astype(BF16)
        lg_src[j] = m_s[j] + jnp.log(l_s[j])
        kept = (block_of(j) == sp) & primary

        @pl.when(jnp.logical_not(kept))
        def _():
            o_copy(j).start()
            lg_copy(j).start()

        @pl.when(kept)
        def _():
            o_in[src_head] = o_src[j]
            lg_in[src_head] = lg_src[j]

    take_keys(0)
    for j in range(heads):
        if j + 1 < heads:
            take_keys(j + 1)
        if j == heads - 1:
            chain_at(z == 1)
            take_values(0)
        weigh(j)
    for j in range(heads):
        if j + 1 < heads:
            take_values(j + 1)
        finish(j)
    chain_at(z >= 2)

    for j in range(rec_heads):
        lanes = slice(j * STATE_ROWS, (j + 1) * STATE_ROWS)
        out = inner[:, lanes] + dot_nt(vq[:, lanes], incoming[j])
        mean = jnp.mean(out * out, axis=-1, keepdims=True)
        out = out * lax.rsqrt(mean + EPSILON) * r_gain[:, lanes] * og[:, lanes]
        vq[:, lanes] = out.astype(BF16)
    loads[9].wait()
    rec_part[...] = dot(vq[...], wro_v[...])
    loads[8].wait()

    for i in range(heads):
        kept = (home_of(i, my_home) == sp) & (my_core == core)

        @pl.when(jnp.logical_not(kept))
        def _():
            remote(
                o_in.at[i], o_in.at[i], o_send.at[0], o_recv.at[i], (sp, partner)
            ).wait_recv()
            remote(
                lg_in.at[i], lg_in.at[i], lg_send.at[0], lg_recv.at[i], (sp, partner)
            ).wait_recv()

    for i in range(heads):
        logsum_ref[i : i + 1, :] = lg_in[i] + gate_t[i : i + 1, :]
    attn_t = jnp.concatenate([o_in[i].astype(F32) for i in range(heads)], axis=0)
    attn_out = (attn_t.T * a_gain[...]).astype(BF16)

    def rows_of(which_chip, which_core):
        return pl.ds(pl.multiple_of((which_chip * 2 + which_core) * rb, rb), rb)

    def columns(q):
        return slice(q * part_cols, (q + 1) * part_cols)

    def within(j, q):
        return pltpu.make_async_remote_copy(
            src_ref=part.at[q, rows_of(j, 1 - core)], dst_ref=recv1.at[j, q],
            send_sem=s1_send.at[j, q], recv_sem=s1_recv.at[j, q], device_id=(sp, partner),
            device_id_type=MESH,
        )

    def between(j, q):
        return pltpu.make_async_remote_copy(
            src_ref=send2.at[j, q], dst_ref=recv2.at[chip, q], send_sem=s2_send.at[j, q],
            recv_sem=s2_recv.at[chip, q], device_id=(sp, j * 2 + core), device_id_type=MESH,
        )

    order = [(chip + k) % chips for k in range(1, chips)]

    def chip_sum(j, q):
        within(j, q).wait_recv()
        return part[q, rows_of(j, core), :].astype(F32) + recv1[j, q].astype(F32)

    def send_sums(q):
        for j in order:
            send2[j, q] = chip_sum(j, q).astype(BF16)
            between(j, q).start()

    for q in range(splits):
        part[q] = (
            dot(attn_out, wao_v[:, columns(q)]) + rec_part[:, columns(q)]
        ).astype(BF16)
        for j in order:
            within(j, q).start()
        if q > 0:
            send_sums(q - 1)
    send_sums(splits - 1)
    for q in range(splits):
        within(chip, q).start()
    for q in range(splits):
        total = chip_sum(chip, q)
        for j in order:
            pltpu.make_async_remote_copy(
                src_ref=send2.at[j, q], dst_ref=recv2.at[j, q], send_sem=s2_send.at[j, q],
                recv_sem=s2_recv.at[j, q], device_id=(sp, partner), device_id_type=MESH,
            ).wait_recv()
            total = total + recv2[j, q].astype(F32)
        mixed_ref[:, columns(q)] = total.astype(BF16)

    for q in range(splits):
        for j in order + [chip]:
            within(j, q).wait_send()
        for j in order:
            between(j, q).wait_send()
    for k in range(1, ny):
        st_copy(k).wait_send()

    @pl.when(z < nz - 1)
    def _():
        for j in range(rec_heads):
            chain_copy(j).wait_send()

    for i in range(heads):
        for r in range(homes):
            @pl.when(home_of(i, r) != sp)
            def _():
                k_copy(i, r).wait_send()
                v_copy(i, r).wait_send()
                g_copy(i, r, 0).wait_send()

            g_copy(i, r, 1).wait_send()

        @pl.when((home_of(i, my_home) != sp) | (my_core != core))
        def _():
            q_copy(i).wait_send()

    @pl.when(primary)
    def _():
        for t in range(n_sp):
            remote(k_all.at[t], k_all.at[t], k_fwd.at[t], k_recv.at[t], (sp, partner)).wait_send()
            remote(v_all.at[t], v_all.at[t], v_fwd.at[t], v_recv.at[t], (sp, partner)).wait_send()

    for j in range(heads):
        @pl.when((block_of(j) != sp) | jnp.logical_not(primary))
        def _():
            o_copy(j).wait_send()
            lg_copy(j).wait_send()


def body(
    n_sp, n_tp,
    layer_input_rows, input_norm_gain, query_weight, key_weight, value_weight, query_norm_gain,
    key_norm_gain, cumulative_gate, attention_norm_gain, recurrence_query_weight, forget_weight,
    recurrence_value_weight, output_gate_weight, gate_lower_slack, extra_log_decay,
    recurrence_norm_gain, attention_output_weight, recurrence_output_weight,
):
    nz, ny = grid_of(n_sp)
    rows, width = layer_input_rows.shape
    cols = query_weight.shape[1]
    heads, pairs, rec_heads = cols // HEAD_DIM, cols // LANES, cols // STATE_ROWS
    rb, chips = rows // n_tp, n_tp // 2
    half = rows // 2
    homes = n_sp // (2 * heads)
    blocks = 2 * homes * heads * (heads + 1) // 2
    splits = math.gcd(width // LANES, 4)
    weight = pltpu.VMEM((width, cols), BF16)
    two_weights = pltpu.VMEM((width, 2 * cols), BF16)
    out_weight = pltpu.VMEM((cols, width), BF16)
    dma = pltpu.SemaphoreType.DMA
    any_space = pl.BlockSpec(memory_space=pl.ANY)
    vmem = pl.BlockSpec(memory_space=pltpu.VMEM)
    mixed, log_sum = pl.pallas_call(
        functools.partial(kernel, (nz, ny, n_tp)),
        name="mixer",
        out_shape=(
            jax.ShapeDtypeStruct((rb, width), BF16),
            jax.ShapeDtypeStruct((heads, rows), F32),
        ),
        in_specs=[any_space] * 18,
        out_specs=(vmem, vmem),
        scratch_shapes=[
            pltpu.VMEM((rows, width), BF16),
            *([two_weights] * 3), weight, out_weight, out_weight,
            pltpu.VMEM((rows, width), BF16),
            pltpu.VMEM((heads, half, LANES), BF16),
            pltpu.VMEM((heads, HEAD_DIM, rows), BF16),
            pltpu.VMEM((heads, HEAD_DIM, rows), BF16),
            pltpu.VMEM((heads, 1, rows), F32),
            pltpu.VMEM((n_sp, half, LANES), BF16),
            pltpu.VMEM((n_sp, HEAD_DIM, rows), BF16),
            pltpu.VMEM((n_sp, 1, rows), F32),
            pltpu.VMEM((n_sp, half, LANES), BF16),
            pltpu.VMEM((heads, HEAD_DIM, rows), BF16),
            pltpu.VMEM((n_sp, half, 2 * rows), F32),
            pltpu.VMEM((blocks, rows, rows), BF16),
            pltpu.VMEM((heads, 1, rows), F32),
            pltpu.VMEM((heads, 1, rows), F32),
            pltpu.VMEM((heads, HEAD_DIM, rows), BF16),
            pltpu.VMEM((heads, 1, rows), F32),
            pltpu.VMEM((heads, HEAD_DIM, rows), BF16),
            pltpu.VMEM((heads, 1, rows), F32),
            pltpu.VMEM((rows, cols), F32),
            pltpu.VMEM((rows, cols), BF16),
            pltpu.VMEM((rows, cols), F32),
            pltpu.VMEM((8, rows), F32),
            pltpu.VMEM((ny, rec_heads * (STATE_ROWS + 16), STATE_ROWS), BF16),
            *([pltpu.VMEM((rec_heads, STATE_ROWS, STATE_ROWS), BF16)] * 3),
            pltpu.VMEM((splits, rows, width // splits), BF16),
            *([pltpu.VMEM((chips, splits, rb, width // splits), BF16)] * 3),
            *([pltpu.VMEM((1, n), F32) for n in (width, HEAD_DIM, HEAD_DIM)]),
            pltpu.VMEM((heads, rows), F32),
            pltpu.VMEM((1, cols), F32),
            pltpu.VMEM((1, cols), F32),
            pltpu.VMEM((rec_heads, rows), F32),
            pltpu.VMEM((1, cols), F32),
            pltpu.VMEM((rows, width), F32),
            dma((18,)),
            dma((heads, homes)), dma((heads, homes)), dma((heads,)), dma((heads, homes, 2)),
            dma((n_sp,)), dma((n_sp,)), dma((heads,)), dma((n_sp,)), dma((n_sp,)), dma((n_sp,)),
            *([dma((heads,))] * 4),
            *([dma((ny,))] * 2), *([dma((rec_heads,))] * 2),
            *([dma((chips, splits))] * 4),
        ],
        compiler_params=pltpu.CompilerParams(
            collective_id=0, has_side_effects=True, vmem_limit_bytes=48 * 1024 * 1024
        ),
    )(*(pltpu.with_memory_space_constraint(a, pltpu.HBM) for a in (
        layer_input_rows, key_weight, value_weight, forget_weight, recurrence_value_weight,
        recurrence_query_weight, query_weight, output_gate_weight, attention_output_weight,
        recurrence_output_weight,
        input_norm_gain.reshape(1, -1), query_norm_gain.reshape(1, -1),
        key_norm_gain.reshape(1, -1), cumulative_gate.T, attention_norm_gain.reshape(1, -1),
        gate_lower_slack.reshape(1, -1), extra_log_decay.T, recurrence_norm_gain.reshape(1, -1),
        )))
    return mixed, log_sum.T


def solution(mesh):
    return jax.shard_map(
        functools.partial(body, mesh.shape["sp"], mesh.shape["tp"]),
        mesh=mesh,
        in_specs=(
            P("sp", None),
            P(),
            P(None, "tp"),
            P(None, "tp"),
            P(None, "tp"),
            P(),
            P(),
            P("sp", "tp"),
            P("tp"),
            P(None, "tp"),
            P(None, "tp"),
            P(None, "tp"),
            P(None, "tp"),
            P("tp"),
            P("sp", "tp"),
            P("tp"),
            P("tp", None),
            P("tp", None),
        ),
        out_specs=(P(("sp", "tp"), None), P("sp", "tp")),
        check_vma=False,
    )
```

```python
import functools
import math

import jax
import jax.numpy as jnp
from jax import lax
from jax.experimental import pallas as pl
from jax.experimental.pallas import tpu as pltpu
from jax.sharding import PartitionSpec as P

HEAD_DIM = 64
STATE_ROWS = 128
LANES = 128
EPSILON = 1e-06
MESH = pl.DeviceIdType.MESH
F32 = jnp.float32
BF16 = jnp.bfloat16


def dot(a, b):
    return jnp.dot(a, b, preferred_element_type=F32)


def parts_of(a, count):
    parts = []
    for _ in range(count):
        parts.append(a.astype(BF16))
        a = a - parts[-1].astype(F32)
    return parts


def dot_nt(a, b):
    return lax.dot_general(
        a, b, (((1,), (1,)), ((), ())), preferred_element_type=F32
    )


def iota(shape, axis):
    return lax.broadcasted_iota(jnp.int32, shape, axis)


def grid_of(count):
    columns = max(c for c in range(1, math.isqrt(count) + 1) if count % c == 0)
    return count // columns, columns


def kernel(
    sizes,
    x_hbm, wk_hbm, wv_hbm, wf_hbm, wrv_hbm, wrq_hbm, wq_hbm, wog_hbm, wao_hbm, wro_hbm,
    in_gain_hbm, q_gain_hbm, k_gain_hbm, gate_t_hbm, a_gain_hbm,
    slack_hbm, extra_t_hbm, r_gain_hbm,
    mixed_ref, logsum_ref,
    x_v, wkq_v, wfr_v, wvr_v, wog_v, wao_v, wro_v,
    xn, k_src, q_src, v_src, g_src, k_all, v_all, g_all, ga, q_in, s_buf, w_buf, m_s, l_s,
    o_src, lg_src, o_in, lg_in, attn_out,
    inner, vq, og, ext, st, up_in, up_out, chain_in, chain_out, incoming, part, send2, recv1, recv2,
    in_gain, q_gain, k_gain, gate_t, a_gain, slack, extra_t, r_gain, rec_part,
    load_sem, k_send, v_send, q_send, g_send, k_recv, v_recv, q_recv, g_recv, k_fwd, v_fwd,
    o_send, o_recv, lg_send, lg_recv,
    st_send, st_recv, up_send, up_recv, chain_send, chain_recv,
    s1_send, s1_recv, s2_send, s2_recv,
):
    nz, ny, ntp = sizes
    n_sp = nz * ny
    rows, width = x_v.shape
    cols = wog_v.shape[1]
    heads = cols // HEAD_DIM
    pairs = cols // LANES
    rec_heads = cols // STATE_ROWS
    chips = ntp // 2
    rb = rows // ntp
    half = rows // 2
    splits = s1_recv.shape[1]
    part_cols = width // splits
    homes = n_sp // (2 * heads)
    members = 2 * homes

    sp, tp = lax.axis_index("sp"), lax.axis_index("tp")
    z, y = sp // ny, sp % ny
    chip, core = tp // 2, tp % 2
    partner = chip * 2 + (1 - core)

    group = sp // homes
    src_core, src_head = group % 2, group // 2
    primary = core == src_core
    member = (sp % homes) * 2 + core
    src_tp = chip * 2 + src_core

    def block_of(j):
        return j * members + (member if j % 2 == 0 else members - 1 - member)

    my_j = sp // members
    my_u = sp % members
    my_member = my_u + (my_j % 2) * (members - 1 - 2 * my_u)
    my_home, my_core = my_member // 2, my_member % 2

    def home_of(i, r):
        return (2 * i + core) * homes + r

    loads = []
    for i, (src, dst) in enumerate((
        (x_hbm, x_v), (wk_hbm, wkq_v.at[:, 0:cols]), (wq_hbm, wkq_v.at[:, cols : 2 * cols]),
        (wf_hbm, wfr_v.at[:, 0:cols]), (wrv_hbm, wfr_v.at[:, cols : 2 * cols]),
        (wv_hbm, wvr_v.at[:, 0:cols]), (wrq_hbm, wvr_v.at[:, cols : 2 * cols]),
        (wog_hbm, wog_v), (wao_hbm, wao_v), (wro_hbm, wro_v),
        (in_gain_hbm, in_gain), (q_gain_hbm, q_gain), (k_gain_hbm, k_gain),
        (gate_t_hbm, gate_t), (a_gain_hbm, a_gain), (slack_hbm, slack),
        (extra_t_hbm, extra_t), (r_gain_hbm, r_gain),
    )):
        loads.append(pltpu.make_async_copy(src, dst, load_sem.at[i - 1 if i in (2, 4, 6) else i]))

    for copy in loads[:1] + loads[10:] + loads[1:3]:
        copy.start()

    def both(ref, i):
        pltpu.make_async_copy(ref, ref, load_sem.at[i]).wait()

    barrier = pltpu.get_barrier_semaphore()

    def greet(where):
        pl.semaphore_signal(barrier, inc=1, device_id=where, device_id_type=MESH)

    for k in range(n_sp):
        if k > 0:
            greet(((sp + k) % n_sp, tp))
        greet(((sp + k) % n_sp, partner))
    for k in range(1, chips):
        greet((sp, ((chip + k) % chips) * 2 + core))

    loads[0].wait()
    for copy in loads[10:]:
        copy.wait()
    for copy in loads[3:5]:
        copy.start()
    xf = x_v[...].astype(F32)
    scale = lax.rsqrt(jnp.mean(xf * xf, axis=-1, keepdims=True) + EPSILON)
    xn[...] = (xf * scale * in_gain[...]).astype(BF16)

    for i in range(heads):
        g_src[i] = gate_t[i : i + 1, :]

    block_ones = jnp.where(
        iota((cols, cols), 0) // HEAD_DIM == iota((cols, cols), 1) // HEAD_DIM, 1.0 / HEAD_DIM, 0.0
    ).astype(BF16)

    def head_norm(v, gain_ref):
        mean = sum(dot(p, block_ones) for p in parts_of(v * v, 2))
        gain = jnp.concatenate([gain_ref[...]] * heads, axis=1)
        return v * lax.rsqrt(mean + EPSILON) * gain

    both(wkq_v, 1)
    for copy in loads[5:7]:
        copy.start()
    kq = dot(xn[...], wkq_v[...])
    keys = head_norm(kq[:, 0:cols], k_gain)
    first_half = iota((half, LANES), 1) < HEAD_DIM
    for p in range(pairs):
        low = keys[0:half, p * LANES : (p + 1) * LANES]
        high = keys[half:rows, p * LANES : (p + 1) * LANES]
        k_src[2 * p] = jnp.where(first_half, low, pltpu.roll(high, HEAD_DIM, 1)).astype(BF16)
        k_src[2 * p + 1] = jnp.where(first_half, pltpu.roll(low, HEAD_DIM, 1), high).astype(BF16)
    queries_t = (head_norm(kq[:, cols : 2 * cols], q_gain).astype(BF16).astype(F32)).T
    for i in range(heads):
        q_src[i] = (queries_t[i * HEAD_DIM : (i + 1) * HEAD_DIM, :] * HEAD_DIM ** (-0.5)).astype(BF16)

    def remote(src, dst, send, recv, where):
        return pltpu.make_async_remote_copy(
            src_ref=src, dst_ref=dst, send_sem=send, recv_sem=recv,
            device_id=where, device_id_type=MESH,
        )

    def k_copy(i, r):
        return remote(
            k_src.at[i], k_all.at[sp], k_send, k_recv.at[my_j], (home_of(i, r), tp)
        )

    def v_copy(i, r):
        return remote(
            v_src.at[i], v_all.at[sp], v_send, v_recv.at[my_j], (home_of(i, r), tp)
        )

    def g_copy(i, r, c):
        return remote(
            g_src.at[i], g_all.at[sp], g_send, g_recv, (home_of(i, r), tp if c == 0 else partner)
        )

    def q_copy(i):
        return remote(
            q_src.at[i], q_in.at[my_j], q_send, q_recv.at[my_j],
            (home_of(i, my_home), chip * 2 + my_core),
        )

    def sent(ref, sem):
        remote(ref, ref, sem, g_recv, (sp, partner)).wait_send()

    def landed(ref, sem):
        remote(ref, ref, g_send, sem, (sp, partner)).wait_recv()

    def either(here, act, ref, few, many):
        @pl.when(here)
        def _():
            act(ref.at[0:few])

        @pl.when(jnp.logical_not(here))
        def _():
            act(ref.at[0:many])

    own = primary & (member == my_member)

    turns = [(src_head + k) % heads for k in range(heads)]

    def spread(copies, local):
        for i in turns:
            for r in range(homes):
                @pl.when(home_of(i, r) != sp)
                def _():
                    copies(i, r).start()

                @pl.when(home_of(i, r) == sp)
                def _():
                    local(i)

    def keep_k(i):
        k_all[sp] = k_src[i]

    def keep_v(i):
        v_all[sp] = v_src[i]

    def keep_g(i):
        g_all[sp] = g_src[i]

    def begin():
        pl.semaphore_wait(barrier, 2 * n_sp - 1 + chips - 1)

    def send_keys_and_queries():
        spread(lambda i, r: g_copy(i, r, 0), keep_g)
        for i in range(heads):
            for r in range(homes):
                g_copy(i, r, 1).start()
        spread(k_copy, keep_k)
        for i in turns:
            stays = own & (i == src_head)

            @pl.when(jnp.logical_not(stays))
            def _():
                q_copy(i).start()

            @pl.when(stays)
            def _():
                q_in[my_j] = q_src[i]

    early = z == 0

    @pl.when(jnp.logical_not(early))
    def _():
        begin()
        send_keys_and_queries()

    tri = iota((rows, rows), 0) >= iota((rows, rows), 1)
    tri_b = tri.astype(F32).astype(BF16)
    both(wfr_v, 3)
    for copy in loads[7:10]:
        copy.start()
    fr = dot(xn[...], wfr_v[...])
    share = slack[...] / (1.0 + jnp.exp(fr[:, 0:cols]))
    rec_value = fr[:, cols : 2 * cols]
    run = sum(dot(tri_b, p) for p in parts_of(jnp.log1p(-share), 3))
    ext[...] = jnp.zeros_like(ext)
    ext[0:rec_heads, :] = extra_t[...]
    ext_row = sum(dot_nt(p, tri_b) for p in parts_of(ext[...], 3))
    ext_col = ext_row.T
    last = run[rows - 1 : rows]
    st_rows = STATE_ROWS + 16
    for j in range(rec_heads):
        lanes = slice(j * STATE_ROWS, (j + 1) * STATE_ROWS)
        e_col = ext_col[:, j : j + 1]
        e_row = ext_row[j : j + 1, :]
        e_last = e_row[:, rows - 1 : rows]
        left = share[:, lanes] * jnp.exp(last[:, lanes] - run[:, lanes] + (e_last - e_col))
        st[y, j * st_rows : j * st_rows + STATE_ROWS, :] = dot(
            rec_value[:, lanes].T.astype(BF16), left.astype(BF16)
        ).astype(BF16)
        st[y, j * st_rows + STATE_ROWS : (j + 1) * st_rows, :] = jnp.broadcast_to(
            jnp.exp(last[:, lanes] + e_last), (16, STATE_ROWS)
        ).astype(BF16)

    def st_copy(k):
        return remote(
            st.at[y], st.at[y], st_send, st_recv, (z * ny + (y + k) % ny, tp)
        )

    lifts = (z % 2 == 0) & (z + 1 < nz)

    @pl.when(early)
    def _():
        begin()

    for k in range(1, ny):
        st_copy(k).start()

    @pl.when(early)
    def _():
        send_keys_and_queries()

    both(wvr_v, 5)
    vr = dot(xn[...], wvr_v[...])
    values_t = vr[:, 0:cols].T.astype(BF16)
    for i in range(heads):
        v_src[i] = values_t[i * HEAD_DIM : (i + 1) * HEAD_DIM, :]
    spread(v_copy, keep_v)

    rec_query = vr[:, cols : 2 * cols]
    rec_query = rec_query / (1.0 + jnp.exp(-rec_query))
    grown = rec_query * jnp.exp(run)
    for j in range(rec_heads):
        lanes = slice(j * STATE_ROWS, (j + 1) * STATE_ROWS)
        e_col = ext_col[:, j : j + 1]
        e_row = ext_row[j : j + 1, :]
        value = rec_value[:, lanes].astype(BF16)
        scores = dot_nt(
            grown[:, lanes].astype(BF16), (share[:, lanes] * jnp.exp(-run[:, lanes])).astype(BF16)
        )
        fading = jnp.exp(jnp.where(tri, e_col - e_row, -jnp.inf))
        scores = jnp.where(tri, scores * fading, 0.0)
        inner[:, lanes] = dot(scores.astype(BF16), value)
        vq[:, lanes] = (grown[:, lanes] * jnp.exp(e_col)).astype(BF16)

    loads[7].wait()
    gate_out = dot(xn[...], wog_v[...])
    og[...] = gate_out / (1.0 + jnp.exp(-gate_out))

    def up_copy(j):
        return remote(
            up_out.at[j], up_in.at[j], up_send, up_recv.at[j], ((sp + ny) % n_sp, tp)
        )

    def chain_copy(j, d):
        return remote(
            chain_out.at[j], chain_in.at[j], chain_send.at[d - 1], chain_recv.at[j],
            ((sp + d * ny) % n_sp, tp),
        )

    def added(j, k):
        base = j * st_rows
        return (
            st[k, base : base + STATE_ROWS, :].astype(F32),
            st[k, base + STATE_ROWS : base + st_rows, :].astype(F32),
        )

    def states_of_row():
        if ny > 1:
            landed(st.at[0 : ny - 1], st_recv)

    def lift():
        for j in range(rec_heads):
            total, kept = added(j, 0)
            for k in range(1, ny):
                more, decay = added(j, k)
                total, kept = total * decay[0:1] + more, kept * decay
            up_out[j, 0:STATE_ROWS, :] = total.astype(BF16)
            up_out[j, STATE_ROWS:st_rows, :] = kept.astype(BF16)
            up_copy(j).start()

    def advance(received, odd):
        for j in range(rec_heads):
            state = jnp.zeros((STATE_ROWS, STATE_ROWS), F32)
            if received:
                landed(chain_in.at[j], chain_recv.at[j])
                state = chain_in[j].astype(F32)
            if odd:
                landed(up_in.at[j], up_recv.at[j])
                decay = up_in[j, STATE_ROWS:st_rows, :].astype(F32)[0:1]
                state = state * decay + up_in[j, 0:STATE_ROWS, :].astype(F32)
            for k in range(ny):
                @pl.when(y == k)
                def _():
                    incoming[j] = state.astype(BF16)

                if odd or k + 1 < ny:
                    more, decay = added(j, k)
                    state = state * decay[0:1] + more
            if odd:
                chain_out[j] = state.astype(BF16)
                for d in (1, 2):
                    @pl.when(z + d < nz)
                    def _():
                        chain_copy(j, d).start()

    def advance_at(where, received, odd):
        @pl.when(where & (z % 2 == odd))
        def _():
            advance(received, odd)

    states_of_row()

    @pl.when(lifts)
    def _():
        lift()

    advance_at(z < 2, False, 0)

    either(primary, lambda ref: landed(ref, g_recv), g_all, n_sp - 1, n_sp)

    gate_cols = jnp.concatenate(
        [g_all[t, :, h * half : (h + 1) * half] for t in range(n_sp) for h in range(2)], axis=0
    ).T
    gate_parts = jnp.concatenate(
        [p.astype(F32) for p in parts_of(gate_cols, 3)]
        + [jnp.zeros((half, LANES - 6 * n_sp), F32)] * (6 * n_sp < LANES), axis=1
    )
    lane_block = (iota((half, LANES), 1) % (2 * n_sp)) // 2
    for t in range(n_sp):
        ga[t] = jnp.where(lane_block == t, gate_parts, 0.0).astype(BF16)

    def take(ref, fwd, recv, j):
        either(
            primary & (my_j == j), lambda part: landed(part, recv.at[j]), ref,
            members - 1, members,
        )

        @pl.when(primary)
        def _():
            for t in range(j * members, (j + 1) * members):
                remote(ref.at[t], ref.at[t], fwd, recv.at[j], (sp, partner)).start()

    def take_keys(j):
        take(k_all, k_fwd, k_recv, j)

    def take_values(j):
        take(v_all, v_fwd, v_recv, j)

    minus = jnp.where(
        iota((LANES, 2 * rows), 0) % 2 == iota((LANES, 2 * rows), 1) // rows, -1.0, 0.0
    ).astype(BF16)
    ahead = (
        iota((half, 2 * rows), 0) + half * (iota((half, 2 * rows), 1) // rows)
        - iota((half, 2 * rows), 1) % rows
    )
    first = [members * j * (j + 1) // 2 for j in range(heads)]

    def weigh(j):
        @pl.when(jnp.logical_not(own & (my_j == j)))
        def _():
            landed(q_in.at[j], q_recv.at[j])

        q = q_in[j]
        none = jnp.zeros_like(q)
        right = jnp.concatenate(
            [jnp.concatenate([q, none], axis=1), jnp.concatenate([none, q], axis=1), minus], axis=0
        )
        top = None
        for t in range((j + 1) * members):
            s = dot(jnp.concatenate([k_all[t], ga[t]], axis=1), right)
            if t >= j * members:
                s = jnp.where(ahead <= (block_of(j) - t) * rows, s, -jnp.inf)
            s_buf[t] = s
            here = jnp.max(s, axis=0, keepdims=True)
            top = here if top is None else jnp.maximum(top, here)
        top = jnp.maximum(top[:, 0:rows], top[:, rows : 2 * rows])
        m_s[j] = top
        top = jnp.concatenate([top, top], axis=1)
        total = None
        for t in range((j + 1) * members):
            w = jnp.exp(s_buf[t] - top)
            here = jnp.sum(w, axis=0, keepdims=True)
            total = here if total is None else total + here
            w = w.astype(BF16)
            w_buf[first[j] + t, 0:half, :] = w[:, 0:rows]
            w_buf[first[j] + t, half:rows, :] = w[:, rows : 2 * rows]
        l_s[j] = total[:, 0:rows] + total[:, rows : 2 * rows]

    def o_copy(j):
        return remote(
            o_src.at[j], o_in.at[src_head], o_send, o_recv, (block_of(j), src_tp)
        )

    def lg_copy(j):
        return remote(
            lg_src.at[j], lg_in.at[src_head], lg_send, lg_recv, (block_of(j), src_tp)
        )

    def finish(j):
        n = (j + 1) * members
        summed = [
            sum(dot(v_all[t], w_buf[first[j] + t]) for t in range(u, n, 2)) for u in range(2)
        ]
        out = (summed[0] + summed[1]) / l_s[j]
        mean = jnp.mean(out * out, axis=0, keepdims=True)
        o_src[j] = (out * lax.rsqrt(mean + EPSILON)).astype(BF16)
        lg_src[j] = m_s[j] + jnp.log(l_s[j])
        kept = own & (my_j == j)

        @pl.when(jnp.logical_not(kept))
        def _():
            o_copy(j).start()
            lg_copy(j).start()

        @pl.when(kept)
        def _():
            o_in[src_head] = o_src[j]
            lg_in[src_head] = lg_src[j]

    def finish_next(j):
        take_values(j)
        finish(j)

    lag = 2
    take_keys(0)
    for j in range(heads):
        if j + 1 < heads:
            take_keys(j + 1)
        weigh(j)
        if j + 1 == max(heads - 1, 1):
            advance_at(z < 2, False, 1)
        if j >= lag:
            finish_next(j - lag)
    for j in range(max(heads - lag, 0), heads):
        finish_next(j)
    advance_at(z >= 2, True, 0)
    advance_at(z >= 2, True, 1)

    for j in range(rec_heads):
        lanes = slice(j * STATE_ROWS, (j + 1) * STATE_ROWS)
        out = inner[:, lanes] + dot_nt(vq[:, lanes], incoming[j])
        mean = jnp.mean(out * out, axis=-1, keepdims=True)
        out = out * lax.rsqrt(mean + EPSILON) * r_gain[:, lanes] * og[:, lanes]
        vq[:, lanes] = out.astype(BF16)
    loads[9].wait()
    rec_part[...] = dot(vq[...], wro_v[...])
    loads[8].wait()

    either(own, lambda ref: landed(ref, o_recv), o_in, heads - 1, heads)
    either(own, lambda ref: landed(ref, lg_recv), lg_in, heads - 1, heads)

    for i in range(heads):
        logsum_ref[i : i + 1, :] = lg_in[i] + gate_t[i : i + 1, :]
    attn_t = jnp.concatenate([o_in[i].astype(F32) for i in range(heads)], axis=0)
    attn_out[...] = (attn_t.T * a_gain[...]).astype(BF16)

    def rows_of(which_chip, which_core):
        return pl.ds(pl.multiple_of((which_chip * 2 + which_core) * rb, rb), rb)

    def columns(q):
        return slice(q * part_cols, (q + 1) * part_cols)

    def within(j, q):
        return pltpu.make_async_remote_copy(
            src_ref=part.at[q, rows_of(j, 1 - core)], dst_ref=recv1.at[j, q],
            send_sem=s1_send, recv_sem=s1_recv.at[j, q], device_id=(sp, partner),
            device_id_type=MESH,
        )

    def between(j, q):
        return pltpu.make_async_remote_copy(
            src_ref=send2.at[j, q], dst_ref=recv2.at[chip, q], send_sem=s2_send,
            recv_sem=s2_recv.at[chip, q], device_id=(sp, j * 2 + core), device_id_type=MESH,
        )

    order = [(chip + k) % chips for k in range(1, chips)]

    def chip_sum(j, q):
        within(j, q).wait_recv()
        return part[q, rows_of(j, core), :].astype(F32) + recv1[j, q].astype(F32)

    def send_sums(q):
        for j in order:
            send2[j, q] = chip_sum(j, q).astype(BF16)
            between(j, q).start()

    def partial_of(j, q):
        at = pl.ds(pl.multiple_of(j * 2 * rb, 2 * rb), 2 * rb)
        part[q, at, :] = (
            dot(attn_out[at, :], wao_v[:, columns(q)]) + rec_part[at, columns(q)]
        ).astype(BF16)
        within(j, q).start()

    for q in range(splits):
        for j in order:
            partial_of(j, q)
        if q > 0:
            send_sums(q - 1)
    send_sums(splits - 1)
    for q in range(splits):
        partial_of(chip, q)
    for q in range(splits):
        total = chip_sum(chip, q)
        for j in order:
            pltpu.make_async_remote_copy(
                src_ref=send2.at[j, q], dst_ref=recv2.at[j, q], send_sem=s2_send,
                recv_sem=s2_recv.at[j, q], device_id=(sp, partner), device_id_type=MESH,
            ).wait_recv()
            total = total + recv2[j, q].astype(F32)
        mixed_ref[:, columns(q)] = total.astype(BF16)

    sent(recv1, s1_send)
    if chips > 1:
        sent(recv2.at[0 : chips - 1], s2_send)
    if ny > 1:
        sent(st.at[0 : ny - 1], st_send)

    @pl.when(lifts)
    def _():
        sent(up_out, up_send)

    for d in (1, 2):
        @pl.when((z % 2 == 1) & (z + d < nz))
        def _():
            sent(chain_out, chain_send.at[d - 1])

    copies = heads * homes
    either(primary, lambda ref: sent(ref, k_send), k_all, copies - 1, copies)
    either(primary, lambda ref: sent(ref, v_send), v_all, copies - 1, copies)
    either(primary, lambda ref: sent(ref, g_send), g_all, n_sp - 1, n_sp)
    either(own, lambda ref: sent(ref, q_send), q_in, heads - 1, heads)
    either(own, lambda ref: sent(ref, o_send), o_in, heads - 1, heads)
    either(own, lambda ref: sent(ref, lg_send), lg_in, heads - 1, heads)

    @pl.when(primary)
    def _():
        sent(k_all, k_fwd)
        sent(v_all, v_fwd)


def leave(mixed_v, log_sum_v, mixed_hbm, log_sum_hbm, sem):
    copies = (
        pltpu.make_async_copy(mixed_v, mixed_hbm, sem.at[0]),
        pltpu.make_async_copy(log_sum_v, log_sum_hbm, sem.at[1]),
    )
    for copy in copies:
        copy.start()
    for copy in copies:
        copy.wait()


def body(
    n_sp, n_tp,
    layer_input_rows, input_norm_gain, query_weight, key_weight, value_weight, query_norm_gain,
    key_norm_gain, cumulative_gate, attention_norm_gain, recurrence_query_weight, forget_weight,
    recurrence_value_weight, output_gate_weight, gate_lower_slack, extra_log_decay,
    recurrence_norm_gain, attention_output_weight, recurrence_output_weight,
):
    nz, ny = grid_of(n_sp)
    rows, width = layer_input_rows.shape
    cols = query_weight.shape[1]
    heads, pairs, rec_heads = cols // HEAD_DIM, cols // LANES, cols // STATE_ROWS
    rb, chips = rows // n_tp, n_tp // 2
    half = rows // 2
    homes = n_sp // (2 * heads)
    blocks = 2 * homes * heads * (heads + 1) // 2
    splits = math.gcd(width // LANES, 4)
    weight = pltpu.VMEM((width, cols), BF16)
    two_weights = pltpu.VMEM((width, 2 * cols), BF16)
    out_weight = pltpu.VMEM((cols, width), BF16)
    dma = pltpu.SemaphoreType.DMA
    any_space = pl.BlockSpec(memory_space=pl.ANY)
    vmem = pl.BlockSpec(memory_space=pltpu.VMEM)
    mixed, log_sum = pl.pallas_call(
        functools.partial(kernel, (nz, ny, n_tp)),
        name="mixer",
        out_shape=(
            jax.ShapeDtypeStruct((rb, width), BF16),
            jax.ShapeDtypeStruct((heads, rows), F32),
        ),
        in_specs=[any_space] * 18,
        out_specs=(vmem, vmem),
        scratch_shapes=[
            pltpu.VMEM((rows, width), BF16),
            *([two_weights] * 3), weight, out_weight, out_weight,
            pltpu.VMEM((rows, width), BF16),
            pltpu.VMEM((heads, half, LANES), BF16),
            pltpu.VMEM((heads, HEAD_DIM, rows), BF16),
            pltpu.VMEM((heads, HEAD_DIM, rows), BF16),
            pltpu.VMEM((heads, 1, rows), F32),
            pltpu.VMEM((n_sp, half, LANES), BF16),
            pltpu.VMEM((n_sp, HEAD_DIM, rows), BF16),
            pltpu.VMEM((n_sp, 1, rows), F32),
            pltpu.VMEM((n_sp, half, LANES), BF16),
            pltpu.VMEM((heads, HEAD_DIM, rows), BF16),
            pltpu.VMEM((n_sp, half, 2 * rows), F32),
            pltpu.VMEM((blocks, rows, rows), BF16),
            pltpu.VMEM((heads, 1, rows), F32),
            pltpu.VMEM((heads, 1, rows), F32),
            pltpu.VMEM((heads, HEAD_DIM, rows), BF16),
            pltpu.VMEM((heads, 1, rows), F32),
            pltpu.VMEM((heads, HEAD_DIM, rows), BF16),
            pltpu.VMEM((heads, 1, rows), F32),
            pltpu.VMEM((rows, cols), BF16),
            pltpu.VMEM((rows, cols), F32),
            pltpu.VMEM((rows, cols), BF16),
            pltpu.VMEM((rows, cols), F32),
            pltpu.VMEM((8, rows), F32),
            pltpu.VMEM((ny, rec_heads * (STATE_ROWS + 16), STATE_ROWS), BF16),
            *([pltpu.VMEM((rec_heads, STATE_ROWS + 16, STATE_ROWS), BF16)] * 2),
            *([pltpu.VMEM((rec_heads, STATE_ROWS, STATE_ROWS), BF16)] * 3),
            pltpu.VMEM((splits, rows, width // splits), BF16),
            *([pltpu.VMEM((chips, splits, rb, width // splits), BF16)] * 3),
            *([pltpu.VMEM((1, n), F32) for n in (width, HEAD_DIM, HEAD_DIM)]),
            pltpu.VMEM((heads, rows), F32),
            pltpu.VMEM((1, cols), F32),
            pltpu.VMEM((1, cols), F32),
            pltpu.VMEM((rec_heads, rows), F32),
            pltpu.VMEM((1, cols), F32),
            pltpu.VMEM((rows, width), F32),
            dma((18,)),
            dma, dma, dma, dma,
            *([dma((heads,))] * 3), dma, dma, dma,
            dma, dma, dma, dma,
            dma, dma, dma, dma((rec_heads,)), dma((2,)), dma((rec_heads,)),
            dma, dma((chips, splits)), dma, dma((chips, splits)),
        ],
        compiler_params=pltpu.CompilerParams(
            collective_id=0, has_side_effects=True, vmem_limit_bytes=48 * 1024 * 1024
        ),
    )(*(pltpu.with_memory_space_constraint(a, pltpu.HBM) for a in (
        layer_input_rows, key_weight, value_weight, forget_weight, recurrence_value_weight,
        recurrence_query_weight, query_weight, output_gate_weight, attention_output_weight,
        recurrence_output_weight,
        input_norm_gain.reshape(1, -1), query_norm_gain.reshape(1, -1),
        key_norm_gain.reshape(1, -1), cumulative_gate.T, attention_norm_gain.reshape(1, -1),
        gate_lower_slack.reshape(1, -1), extra_log_decay.T, recurrence_norm_gain.reshape(1, -1),
        )))
    mixed, log_sum = pl.pallas_call(
        leave,
        name="leave",
        out_shape=(
            jax.ShapeDtypeStruct((rb, width), BF16),
            jax.ShapeDtypeStruct((heads, rows), F32),
        ),
        in_specs=[vmem] * 2,
        out_specs=(any_space, any_space),
        scratch_shapes=[dma((2,))],
        compiler_params=pltpu.CompilerParams(vmem_limit_bytes=4 * 1024 * 1024),
    )(mixed, log_sum)
    return mixed, log_sum.T


def solution(mesh):
    return jax.shard_map(
        functools.partial(body, mesh.shape["sp"], mesh.shape["tp"]),
        mesh=mesh,
        in_specs=(
            P("sp", None),
            P(),
            P(None, "tp"),
            P(None, "tp"),
            P(None, "tp"),
            P(),
            P(),
            P("sp", "tp"),
            P("tp"),
            P(None, "tp"),
            P(None, "tp"),
            P(None, "tp"),
            P(None, "tp"),
            P("tp"),
            P("sp", "tp"),
            P("tp"),
            P("tp", None),
            P("tp", None),
        ),
        out_specs=(P(("sp", "tp"), None), P("sp", "tp")),
        check_vma=False,
    )
```

```python
import functools
import math

import jax
import jax.numpy as jnp
from jax import lax
from jax.experimental import pallas as pl
from jax.experimental.pallas import tpu as pltpu
from jax.sharding import PartitionSpec as P

HEAD_DIM = 64
STATE_ROWS = 128
LANES = 128
EPSILON = 1e-06
MESH = pl.DeviceIdType.MESH
F32 = jnp.float32
BF16 = jnp.bfloat16


def dot(a, b):
    return jnp.dot(a, b, preferred_element_type=F32)


def parts_of(a, count):
    parts = []
    for _ in range(count):
        parts.append(a.astype(BF16))
        a = a - parts[-1].astype(F32)
    return parts


def dot_nt(a, b):
    return lax.dot_general(
        a, b, (((1,), (1,)), ((), ())), preferred_element_type=F32
    )


def iota(shape, axis):
    return lax.broadcasted_iota(jnp.int32, shape, axis)


def grid_of(count):
    columns = max(c for c in range(1, math.isqrt(count) + 1) if count % c == 0)
    return count // columns, columns


def kernel(
    sizes,
    x_hbm, wk_hbm, wv_hbm, wf_hbm, wrv_hbm, wrq_hbm, wq_hbm, wog_hbm, wao_hbm, wro_hbm,
    in_gain_hbm, q_gain_hbm, k_gain_hbm, gate_t_hbm, a_gain_hbm,
    slack_hbm, extra_t_hbm, r_gain_hbm,
    mixed_ref, logsum_ref,
    x_v, wkq_v, wfr_v, wvr_v, wog_v, wo_v,
    xn, k_src, q_src, v_src, g_src, k_all, v_all, g_all, ga, q_in, s_buf, w_buf, m_s, l_s,
    o_src, lg_src, o_in, lg_in, mix,
    inner, vq, og, ext, st, up_in, up_out, chain_in, chain_out, incoming, part, send2, recv1, recv2,
    in_gain, q_gain, k_gain, gate_t, a_gain, slack, extra_t, r_gain,
    load_sem, k_send, v_send, q_send, g_send, k_recv, v_recv, q_recv, g_recv, k_fwd, v_fwd,
    o_send, o_recv, lg_send, lg_recv,
    st_send, st_recv, up_send, up_recv, chain_send, chain_recv,
    s1_send, s1_recv, s2_send, s2_recv,
):
    nz, ny, ntp = sizes
    n_sp = nz * ny
    rows, width = x_v.shape
    cols = wog_v.shape[1]
    heads = cols // HEAD_DIM
    pairs = cols // LANES
    rec_heads = cols // STATE_ROWS
    chips = ntp // 2
    rb = rows // ntp
    half = rows // 2
    splits = s1_recv.shape[1]
    part_cols = width // splits
    homes = n_sp // (2 * heads)
    members = 2 * homes

    sp, tp = lax.axis_index("sp"), lax.axis_index("tp")
    z, y = sp // ny, sp % ny
    chip, core = tp // 2, tp % 2
    partner = chip * 2 + (1 - core)

    group = sp // homes
    src_core, src_head = group % 2, group // 2
    primary = core == src_core
    member = (sp % homes) * 2 + core
    src_tp = chip * 2 + src_core

    def block_of(j):
        return j * members + (member if j % 2 == 0 else members - 1 - member)

    my_j = sp // members
    my_u = sp % members
    my_member = my_u + (my_j % 2) * (members - 1 - 2 * my_u)
    my_home, my_core = my_member // 2, my_member % 2

    def home_of(i, r):
        return (2 * i + core) * homes + r

    loads = []
    for i, (src, dst) in enumerate((
        (x_hbm, x_v), (wk_hbm, wkq_v.at[:, 0:cols]), (wq_hbm, wkq_v.at[:, cols : 2 * cols]),
        (wf_hbm, wfr_v.at[:, 0:cols]), (wrv_hbm, wfr_v.at[:, cols : 2 * cols]),
        (wv_hbm, wvr_v.at[:, 0:cols]), (wrq_hbm, wvr_v.at[:, cols : 2 * cols]),
        (wog_hbm, wog_v), (wao_hbm, wo_v.at[0:cols, :]),
        (wro_hbm, wo_v.at[cols : 2 * cols, :]),
        (in_gain_hbm, in_gain), (q_gain_hbm, q_gain), (k_gain_hbm, k_gain),
        (gate_t_hbm, gate_t), (a_gain_hbm, a_gain), (slack_hbm, slack),
        (extra_t_hbm, extra_t), (r_gain_hbm, r_gain),
    )):
        loads.append(pltpu.make_async_copy(src, dst, load_sem.at[i - 1 if i in (4, 6) else i]))

    for copy in loads[:1] + loads[10:] + loads[1:3]:
        copy.start()

    def both(ref, i):
        pltpu.make_async_copy(ref, ref, load_sem.at[i]).wait()

    barrier = pltpu.get_barrier_semaphore()

    def greet(where):
        pl.semaphore_signal(barrier, inc=1, device_id=where, device_id_type=MESH)

    for k in range(n_sp):
        if k > 0:
            greet(((sp + k) % n_sp, tp))
        greet(((sp + k) % n_sp, partner))
    for k in range(1, chips):
        greet((sp, ((chip + k) % chips) * 2 + core))

    loads[0].wait()
    for copy in loads[10:]:
        copy.wait()
    for copy in loads[3:5]:
        copy.start()
    xf = x_v[...].astype(F32)
    scale = lax.rsqrt(jnp.mean(xf * xf, axis=-1, keepdims=True) + EPSILON)
    xn[...] = (xf * scale * in_gain[...]).astype(BF16)

    for i in range(heads):
        g_src[i] = gate_t[i : i + 1, :]

    block_ones = jnp.where(
        iota((cols, cols), 0) // HEAD_DIM == iota((cols, cols), 1) // HEAD_DIM, 1.0 / HEAD_DIM, 0.0
    ).astype(BF16)

    def head_norm(v, gain_ref):
        mean = sum(dot(p, block_ones) for p in parts_of(v * v, 2))
        gain = jnp.concatenate([gain_ref[...]] * heads, axis=1)
        return v * lax.rsqrt(mean + EPSILON) * gain

    def by_halves(lanes):
        w = wkq_v[:, lanes]
        return jnp.concatenate([dot(xn[0:half, :], w), dot(xn[half:rows, :], w)], axis=0)

    loads[1].wait()
    keys = head_norm(by_halves(slice(0, cols)), k_gain)
    first_half = iota((half, LANES), 1) < HEAD_DIM
    for p in range(pairs):
        low = keys[0:half, p * LANES : (p + 1) * LANES]
        high = keys[half:rows, p * LANES : (p + 1) * LANES]
        k_src[2 * p] = jnp.where(first_half, low, pltpu.roll(high, HEAD_DIM, 1)).astype(BF16)
        k_src[2 * p + 1] = jnp.where(first_half, pltpu.roll(low, HEAD_DIM, 1), high).astype(BF16)
    def remote(src, dst, send, recv, where):
        return pltpu.make_async_remote_copy(
            src_ref=src, dst_ref=dst, send_sem=send, recv_sem=recv,
            device_id=where, device_id_type=MESH,
        )

    def k_copy(i, r):
        return remote(
            k_src.at[i], k_all.at[sp], k_send, k_recv.at[my_j], (home_of(i, r), tp)
        )

    def v_copy(i, r):
        return remote(
            v_src.at[i], v_all.at[sp], v_send, v_recv.at[my_j], (home_of(i, r), tp)
        )

    def g_copy(i, r, c):
        return remote(
            g_src.at[i], g_all.at[sp], g_send, g_recv, (home_of(i, r), tp if c == 0 else partner)
        )

    def q_copy(i):
        return remote(
            q_src.at[i], q_in.at[my_j], q_send, q_recv.at[my_j],
            (home_of(i, my_home), chip * 2 + my_core),
        )

    def sent(ref, sem):
        remote(ref, ref, sem, g_recv, (sp, partner)).wait_send()

    def landed(ref, sem):
        remote(ref, ref, g_send, sem, (sp, partner)).wait_recv()

    def either(here, act, ref, few, many):
        @pl.when(here)
        def _():
            act(ref.at[0:few])

        @pl.when(jnp.logical_not(here))
        def _():
            act(ref.at[0:many])

    own = primary & (member == my_member)

    turns = [(src_head + k) % heads for k in range(heads)]

    def spread(copies, local):
        for i in turns:
            for r in range(homes):
                @pl.when(home_of(i, r) != sp)
                def _():
                    copies(i, r).start()

                @pl.when(home_of(i, r) == sp)
                def _():
                    local(i)

    def keep_k(i):
        k_all[sp] = k_src[i]

    def keep_v(i):
        v_all[sp] = v_src[i]

    def keep_g(i):
        g_all[sp] = g_src[i]

    def begin():
        pl.semaphore_wait(barrier, 2 * n_sp - 1 + chips - 1)

    def send_keys():
        spread(lambda i, r: g_copy(i, r, 0), keep_g)
        for i in range(heads):
            for r in range(homes):
                g_copy(i, r, 1).start()
        spread(k_copy, keep_k)

    def send_queries():
        for i in turns:
            stays = own & (i == src_head)

            @pl.when(jnp.logical_not(stays))
            def _():
                q_copy(i).start()

            @pl.when(stays)
            def _():
                q_in[my_j] = q_src[i]

    early = z == 0

    @pl.when(jnp.logical_not(early))
    def _():
        begin()
        send_keys()

    loads[2].wait()
    for copy in loads[5:7]:
        copy.start()
    queries = head_norm(by_halves(slice(cols, 2 * cols)), q_gain)
    queries_t = (queries.astype(BF16).astype(F32) * HEAD_DIM ** (-0.5)).T.astype(BF16)
    for i in range(heads):
        q_src[i] = queries_t[i * HEAD_DIM : (i + 1) * HEAD_DIM, :]

    @pl.when(jnp.logical_not(early))
    def _():
        send_queries()

    tri = iota((rows, rows), 0) >= iota((rows, rows), 1)
    tri_b = tri.astype(F32).astype(BF16)
    both(wfr_v, 3)
    for copy in loads[7:10]:
        copy.start()
    fr = dot(xn[...], wfr_v[...])
    share = slack[...] / (1.0 + jnp.exp(fr[:, 0:cols]))
    rec_value = fr[:, cols : 2 * cols]
    run = sum(dot(tri_b, p) for p in parts_of(jnp.log1p(-share), 3))
    ext[...] = jnp.zeros_like(ext)
    ext[0:rec_heads, :] = extra_t[...]
    ext_row = sum(dot_nt(p, tri_b) for p in parts_of(ext[...], 3))
    ext_col = ext_row.T
    last = run[rows - 1 : rows]
    st_rows = STATE_ROWS + 16
    for j in range(rec_heads):
        lanes = slice(j * STATE_ROWS, (j + 1) * STATE_ROWS)
        e_col = ext_col[:, j : j + 1]
        e_row = ext_row[j : j + 1, :]
        e_last = e_row[:, rows - 1 : rows]
        left = share[:, lanes] * jnp.exp(last[:, lanes] - run[:, lanes] + (e_last - e_col))
        st[y, j * st_rows : j * st_rows + STATE_ROWS, :] = dot(
            rec_value[:, lanes].T.astype(BF16), left.astype(BF16)
        ).astype(BF16)
        st[y, j * st_rows + STATE_ROWS : (j + 1) * st_rows, :] = jnp.broadcast_to(
            jnp.exp(last[:, lanes] + e_last), (16, STATE_ROWS)
        ).astype(BF16)

    def st_copy(k):
        return remote(
            st.at[y], st.at[y], st_send, st_recv, (z * ny + (y + k) % ny, tp)
        )

    lifts = (z % 2 == 0) & (z + 1 < nz)

    @pl.when(early)
    def _():
        begin()

    for k in range(1, ny):
        st_copy(k).start()

    @pl.when(early)
    def _():
        send_keys()
        send_queries()

    both(wvr_v, 5)
    vr = dot(xn[...], wvr_v[...])
    values_t = vr[:, 0:cols].T.astype(BF16)
    for i in range(heads):
        v_src[i] = values_t[i * HEAD_DIM : (i + 1) * HEAD_DIM, :]
    spread(v_copy, keep_v)

    rec_query = vr[:, cols : 2 * cols]
    rec_query = rec_query / (1.0 + jnp.exp(-rec_query))
    grown = rec_query * jnp.exp(run)
    for j in range(rec_heads):
        lanes = slice(j * STATE_ROWS, (j + 1) * STATE_ROWS)
        e_col = ext_col[:, j : j + 1]
        e_row = ext_row[j : j + 1, :]
        value = rec_value[:, lanes].astype(BF16)
        scores = dot_nt(
            grown[:, lanes].astype(BF16), (share[:, lanes] * jnp.exp(-run[:, lanes])).astype(BF16)
        )
        fading = jnp.exp(jnp.where(tri, e_col - e_row, -jnp.inf))
        scores = jnp.where(tri, scores * fading, 0.0)
        inner[:, lanes] = dot(scores.astype(BF16), value)
        vq[:, lanes] = (grown[:, lanes] * jnp.exp(e_col)).astype(BF16)

    loads[7].wait()
    gate_out = dot(xn[...], wog_v[...])
    og[...] = gate_out / (1.0 + jnp.exp(-gate_out))

    def up_copy(j):
        return remote(
            up_out.at[j], up_in.at[j], up_send, up_recv.at[j], ((sp + ny) % n_sp, tp)
        )

    def chain_copy(j, d):
        return remote(
            chain_out.at[j], chain_in.at[j], chain_send.at[d - 1], chain_recv.at[j],
            ((sp + d * ny) % n_sp, tp),
        )

    def added(j, k):
        base = j * st_rows
        return (
            st[k, base : base + STATE_ROWS, :].astype(F32),
            st[k, base + STATE_ROWS : base + st_rows, :].astype(F32),
        )

    def states_of_row():
        if ny > 1:
            landed(st.at[0 : ny - 1], st_recv)

    def lift():
        for j in range(rec_heads):
            total, kept = added(j, 0)
            for k in range(1, ny):
                more, decay = added(j, k)
                total, kept = total * decay[0:1] + more, kept * decay
            up_out[j, 0:STATE_ROWS, :] = total.astype(BF16)
            up_out[j, STATE_ROWS:st_rows, :] = kept.astype(BF16)
            up_copy(j).start()

    def advance(received, odd):
        for j in range(rec_heads):
            state = jnp.zeros((STATE_ROWS, STATE_ROWS), F32)
            if received:
                landed(chain_in.at[j], chain_recv.at[j])
                state = chain_in[j].astype(F32)
            if odd:
                landed(up_in.at[j], up_recv.at[j])
                decay = up_in[j, STATE_ROWS:st_rows, :].astype(F32)[0:1]
                state = state * decay + up_in[j, 0:STATE_ROWS, :].astype(F32)
            for k in range(ny):
                @pl.when(y == k)
                def _():
                    incoming[j] = state.astype(BF16)

                if odd or k + 1 < ny:
                    more, decay = added(j, k)
                    state = state * decay[0:1] + more
            if odd:
                chain_out[j] = state.astype(BF16)
                for d in (1, 2):
                    @pl.when(z + d < nz)
                    def _():
                        chain_copy(j, d).start()

    def advance_at(where, received, odd):
        @pl.when(where & (z % 2 == odd))
        def _():
            advance(received, odd)

    states_of_row()

    @pl.when(lifts)
    def _():
        lift()

    advance_at(z < 2, False, 0)

    either(primary, lambda ref: landed(ref, g_recv), g_all, n_sp - 1, n_sp)

    gate_cols = jnp.concatenate(
        [g_all[t, :, h * half : (h + 1) * half] for t in range(n_sp) for h in range(2)], axis=0
    ).T
    gate_parts = jnp.concatenate(
        [p.astype(F32) for p in parts_of(gate_cols, 3)]
        + [jnp.zeros((half, LANES - 6 * n_sp), F32)] * (6 * n_sp < LANES), axis=1
    )
    lane_block = (iota((half, LANES), 1) % (2 * n_sp)) // 2
    for t in range(n_sp):
        ga[t] = jnp.where(lane_block == t, gate_parts, 0.0).astype(BF16)

    def take(ref, fwd, recv, j):
        either(
            primary & (my_j == j), lambda part: landed(part, recv.at[j]), ref,
            members - 1, members,
        )

        @pl.when(primary)
        def _():
            for t in range(j * members, (j + 1) * members):
                remote(ref.at[t], ref.at[t], fwd, recv.at[j], (sp, partner)).start()

    def take_keys(j):
        take(k_all, k_fwd, k_recv, j)

    def take_values(j):
        take(v_all, v_fwd, v_recv, j)

    minus = jnp.where(
        iota((LANES, 2 * rows), 0) % 2 == iota((LANES, 2 * rows), 1) // rows, -1.0, 0.0
    ).astype(BF16)
    ahead = (
        iota((half, 2 * rows), 0) + half * (iota((half, 2 * rows), 1) // rows)
        - iota((half, 2 * rows), 1) % rows
    )
    first = [members * j * (j + 1) // 2 for j in range(heads)]

    def take_query(j):
        @pl.when(jnp.logical_not(own & (my_j == j)))
        def _():
            landed(q_in.at[j], q_recv.at[j])

    def weigh(j):
        q = q_in[j]
        none = jnp.zeros_like(q)
        right = jnp.concatenate(
            [jnp.concatenate([q, none], axis=1), jnp.concatenate([none, q], axis=1), minus], axis=0
        )
        top = None
        for t in range((j + 1) * members):
            s = dot(jnp.concatenate([k_all[t], ga[t]], axis=1), right)
            if t >= j * members:
                s = jnp.where(ahead <= (block_of(j) - t) * rows, s, -jnp.inf)
            s_buf[t] = s
            here = jnp.max(s, axis=0, keepdims=True)
            top = here if top is None else jnp.maximum(top, here)
        top = jnp.maximum(top[:, 0:rows], top[:, rows : 2 * rows])
        m_s[j] = top
        top = jnp.concatenate([top, top], axis=1)
        total = None
        for t in range((j + 1) * members):
            w = jnp.exp(s_buf[t] - top)
            here = jnp.sum(w, axis=0, keepdims=True)
            total = here if total is None else total + here
            w = w.astype(BF16)
            w_buf[first[j] + t, 0:half, :] = w[:, 0:rows]
            w_buf[first[j] + t, half:rows, :] = w[:, rows : 2 * rows]
        l_s[j] = total[:, 0:rows] + total[:, rows : 2 * rows]

    def o_copy(j):
        return remote(
            o_src.at[j], o_in.at[src_head], o_send, o_recv, (block_of(j), src_tp)
        )

    def lg_copy(j):
        return remote(
            lg_src.at[j], lg_in.at[src_head], lg_send, lg_recv, (block_of(j), src_tp)
        )

    def finish(j):
        n = (j + 1) * members
        summed = [
            sum(dot(v_all[t], w_buf[first[j] + t]) for t in range(u, n, 2)) for u in range(2)
        ]
        out = (summed[0] + summed[1]) / l_s[j]
        mean = jnp.mean(out * out, axis=0, keepdims=True)
        o_src[j] = (out * lax.rsqrt(mean + EPSILON)).astype(BF16)
        lg_src[j] = m_s[j] + jnp.log(l_s[j])

    def give(j):
        kept = own & (my_j == j)

        @pl.when(jnp.logical_not(kept))
        def _():
            o_copy(j).start()
            lg_copy(j).start()

        @pl.when(kept)
        def _():
            o_in[src_head] = o_src[j]
            lg_in[src_head] = lg_src[j]

    def each(jobs, *acts):
        for act in acts:
            for j in jobs:
                act(j)

    at = max(heads - 2, 1)
    each(range(at), take_keys, take_query, weigh)
    each(range(at, heads), take_keys, take_query)
    advance_at(z < 2, False, 1)
    each((0,), take_values, finish, give)
    each(range(at, heads), weigh)
    each(range(1, heads - 1), take_values, finish, give)
    each((heads - 1,), take_values, finish, give)
    advance_at(z >= 2, True, 0)
    advance_at(z >= 2, True, 1)

    for j in range(rec_heads):
        lanes = slice(j * STATE_ROWS, (j + 1) * STATE_ROWS)
        out = inner[:, lanes] + dot_nt(vq[:, lanes], incoming[j])
        mean = jnp.mean(out * out, axis=-1, keepdims=True)
        out = out * lax.rsqrt(mean + EPSILON) * r_gain[:, lanes] * og[:, lanes]
        mix[:, cols + j * STATE_ROWS : cols + (j + 1) * STATE_ROWS] = out.astype(BF16)
    loads[9].wait()
    loads[8].wait()

    either(own, lambda ref: landed(ref, o_recv), o_in, heads - 1, heads)
    either(own, lambda ref: landed(ref, lg_recv), lg_in, heads - 1, heads)

    for i in range(heads):
        logsum_ref[i : i + 1, :] = lg_in[i] + gate_t[i : i + 1, :]
    attn_t = jnp.concatenate([o_in[i].astype(F32) for i in range(heads)], axis=0)
    mix[:, 0:cols] = (attn_t.T * a_gain[...]).astype(BF16)

    def rows_of(which_chip, which_core):
        return pl.ds(pl.multiple_of((which_chip * 2 + which_core) * rb, rb), rb)

    def columns(q):
        return slice(q * part_cols, (q + 1) * part_cols)

    def within(j, q):
        return pltpu.make_async_remote_copy(
            src_ref=part.at[q, rows_of(j, 1 - core)], dst_ref=recv1.at[j, q],
            send_sem=s1_send, recv_sem=s1_recv.at[j, q], device_id=(sp, partner),
            device_id_type=MESH,
        )

    def between(j, q):
        return pltpu.make_async_remote_copy(
            src_ref=send2.at[j, q], dst_ref=recv2.at[chip, q], send_sem=s2_send,
            recv_sem=s2_recv.at[chip, q], device_id=(sp, j * 2 + core), device_id_type=MESH,
        )

    order = [(chip + k) % chips for k in range(1, chips)]

    def chip_sum(j, q):
        within(j, q).wait_recv()
        return part[q, rows_of(j, core), :].astype(F32) + recv1[j, q].astype(F32)

    def send_sums(q):
        for j in order:
            send2[j, q] = chip_sum(j, q).astype(BF16)
            between(j, q).start()

    def partial_of(j, q):
        at = pl.ds(pl.multiple_of(j * 2 * rb, 2 * rb), 2 * rb)
        part[q, at, :] = dot(mix[at, :], wo_v[:, columns(q)]).astype(BF16)
        within(j, q).start()

    for q in range(splits):
        for j in order:
            partial_of(j, q)
        if q > 0:
            send_sums(q - 1)
    send_sums(splits - 1)
    for q in range(splits):
        partial_of(chip, q)
    for q in range(splits):
        total = chip_sum(chip, q)
        for j in order:
            pltpu.make_async_remote_copy(
                src_ref=send2.at[j, q], dst_ref=recv2.at[j, q], send_sem=s2_send,
                recv_sem=s2_recv.at[j, q], device_id=(sp, partner), device_id_type=MESH,
            ).wait_recv()
            total = total + recv2[j, q].astype(F32)
        mixed_ref[:, columns(q)] = total.astype(BF16)

    sent(recv1, s1_send)
    if chips > 1:
        sent(recv2.at[0 : chips - 1], s2_send)
    if ny > 1:
        sent(st.at[0 : ny - 1], st_send)

    @pl.when(lifts)
    def _():
        sent(up_out, up_send)

    for d in (1, 2):
        @pl.when((z % 2 == 1) & (z + d < nz))
        def _():
            sent(chain_out, chain_send.at[d - 1])

    copies = heads * homes
    either(primary, lambda ref: sent(ref, k_send), k_all, copies - 1, copies)
    either(primary, lambda ref: sent(ref, v_send), v_all, copies - 1, copies)
    either(primary, lambda ref: sent(ref, g_send), g_all, n_sp - 1, n_sp)
    either(own, lambda ref: sent(ref, q_send), q_in, heads - 1, heads)
    either(own, lambda ref: sent(ref, o_send), o_in, heads - 1, heads)
    either(own, lambda ref: sent(ref, lg_send), lg_in, heads - 1, heads)

    @pl.when(primary)
    def _():
        sent(k_all, k_fwd)
        sent(v_all, v_fwd)


def leave(mixed_v, log_sum_v, mixed_hbm, log_sum_hbm, sem):
    copies = (
        pltpu.make_async_copy(mixed_v, mixed_hbm, sem.at[0]),
        pltpu.make_async_copy(log_sum_v, log_sum_hbm, sem.at[1]),
    )
    for copy in copies:
        copy.start()
    for copy in copies:
        copy.wait()


def body(
    n_sp, n_tp,
    layer_input_rows, input_norm_gain, query_weight, key_weight, value_weight, query_norm_gain,
    key_norm_gain, cumulative_gate, attention_norm_gain, recurrence_query_weight, forget_weight,
    recurrence_value_weight, output_gate_weight, gate_lower_slack, extra_log_decay,
    recurrence_norm_gain, attention_output_weight, recurrence_output_weight,
):
    nz, ny = grid_of(n_sp)
    rows, width = layer_input_rows.shape
    cols = query_weight.shape[1]
    heads, pairs, rec_heads = cols // HEAD_DIM, cols // LANES, cols // STATE_ROWS
    rb, chips = rows // n_tp, n_tp // 2
    half = rows // 2
    homes = n_sp // (2 * heads)
    blocks = 2 * homes * heads * (heads + 1) // 2
    splits = math.gcd(width // LANES, 4)
    weight = pltpu.VMEM((width, cols), BF16)
    two_weights = pltpu.VMEM((width, 2 * cols), BF16)
    dma = pltpu.SemaphoreType.DMA
    any_space = pl.BlockSpec(memory_space=pl.ANY)
    vmem = pl.BlockSpec(memory_space=pltpu.VMEM)
    mixed, log_sum = pl.pallas_call(
        functools.partial(kernel, (nz, ny, n_tp)),
        name="mixer",
        out_shape=(
            jax.ShapeDtypeStruct((rb, width), BF16),
            jax.ShapeDtypeStruct((heads, rows), F32),
        ),
        in_specs=[any_space] * 18,
        out_specs=(vmem, vmem),
        scratch_shapes=[
            pltpu.VMEM((rows, width), BF16),
            *([two_weights] * 3), weight, pltpu.VMEM((2 * cols, width), BF16),
            pltpu.VMEM((rows, width), BF16),
            pltpu.VMEM((heads, half, LANES), BF16),
            pltpu.VMEM((heads, HEAD_DIM, rows), BF16),
            pltpu.VMEM((heads, HEAD_DIM, rows), BF16),
            pltpu.VMEM((heads, 1, rows), F32),
            pltpu.VMEM((n_sp, half, LANES), BF16),
            pltpu.VMEM((n_sp, HEAD_DIM, rows), BF16),
            pltpu.VMEM((n_sp, 1, rows), F32),
            pltpu.VMEM((n_sp, half, LANES), BF16),
            pltpu.VMEM((heads, HEAD_DIM, rows), BF16),
            pltpu.VMEM((n_sp, half, 2 * rows), F32),
            pltpu.VMEM((blocks, rows, rows), BF16),
            pltpu.VMEM((heads, 1, rows), F32),
            pltpu.VMEM((heads, 1, rows), F32),
            pltpu.VMEM((heads, HEAD_DIM, rows), BF16),
            pltpu.VMEM((heads, 1, rows), F32),
            pltpu.VMEM((heads, HEAD_DIM, rows), BF16),
            pltpu.VMEM((heads, 1, rows), F32),
            pltpu.VMEM((rows, 2 * cols), BF16),
            pltpu.VMEM((rows, cols), F32),
            pltpu.VMEM((rows, cols), BF16),
            pltpu.VMEM((rows, cols), F32),
            pltpu.VMEM((8, rows), F32),
            pltpu.VMEM((ny, rec_heads * (STATE_ROWS + 16), STATE_ROWS), BF16),
            *([pltpu.VMEM((rec_heads, STATE_ROWS + 16, STATE_ROWS), BF16)] * 2),
            *([pltpu.VMEM((rec_heads, STATE_ROWS, STATE_ROWS), BF16)] * 3),
            pltpu.VMEM((splits, rows, width // splits), BF16),
            *([pltpu.VMEM((chips, splits, rb, width // splits), BF16)] * 3),
            *([pltpu.VMEM((1, n), F32) for n in (width, HEAD_DIM, HEAD_DIM)]),
            pltpu.VMEM((heads, rows), F32),
            pltpu.VMEM((1, cols), F32),
            pltpu.VMEM((1, cols), F32),
            pltpu.VMEM((rec_heads, rows), F32),
            pltpu.VMEM((1, cols), F32),
            dma((18,)),
            dma, dma, dma, dma,
            *([dma((heads,))] * 3), dma, dma, dma,
            dma, dma, dma, dma,
            dma, dma, dma, dma((rec_heads,)), dma((2,)), dma((rec_heads,)),
            dma, dma((chips, splits)), dma, dma((chips, splits)),
        ],
        compiler_params=pltpu.CompilerParams(
            collective_id=0, has_side_effects=True, vmem_limit_bytes=48 * 1024 * 1024
        ),
    )(*(pltpu.with_memory_space_constraint(a, pltpu.HBM) for a in (
        layer_input_rows, key_weight, value_weight, forget_weight, recurrence_value_weight,
        recurrence_query_weight, query_weight, output_gate_weight, attention_output_weight,
        recurrence_output_weight,
        input_norm_gain.reshape(1, -1), query_norm_gain.reshape(1, -1),
        key_norm_gain.reshape(1, -1), cumulative_gate.T, attention_norm_gain.reshape(1, -1),
        gate_lower_slack.reshape(1, -1), extra_log_decay.T, recurrence_norm_gain.reshape(1, -1),
        )))
    mixed, log_sum = pl.pallas_call(
        leave,
        name="leave",
        out_shape=(
            jax.ShapeDtypeStruct((rb, width), BF16),
            jax.ShapeDtypeStruct((heads, rows), F32),
        ),
        in_specs=[vmem] * 2,
        out_specs=(any_space, any_space),
        scratch_shapes=[dma((2,))],
        compiler_params=pltpu.CompilerParams(vmem_limit_bytes=4 * 1024 * 1024),
    )(mixed, log_sum)
    return mixed, log_sum.T


def solution(mesh):
    return jax.shard_map(
        functools.partial(body, mesh.shape["sp"], mesh.shape["tp"]),
        mesh=mesh,
        in_specs=(
            P("sp", None),
            P(),
            P(None, "tp"),
            P(None, "tp"),
            P(None, "tp"),
            P(),
            P(),
            P("sp", "tp"),
            P("tp"),
            P(None, "tp"),
            P(None, "tp"),
            P(None, "tp"),
            P(None, "tp"),
            P("tp"),
            P("sp", "tp"),
            P("tp"),
            P("tp", None),
            P("tp", None),
        ),
        out_specs=(P(("sp", "tp"), None), P("sp", "tp")),
        check_vma=False,
    )
```

```python
import functools
import math

import jax
import jax.numpy as jnp
from jax import lax
from jax.experimental import pallas as pl
from jax.experimental.pallas import tpu as pltpu
from jax.sharding import PartitionSpec as P

HEAD_DIM = 64
STATE_ROWS = 128
LANES = 128
EPSILON = 1e-06
MESH = pl.DeviceIdType.MESH
F32 = jnp.float32
BF16 = jnp.bfloat16


def dot(a, b):
    return jnp.dot(a, b, preferred_element_type=F32)


def parts_of(a, count):
    parts = []
    for _ in range(count):
        parts.append(a.astype(BF16))
        a = a - parts[-1].astype(F32)
    return parts


def dot_nt(a, b):
    return lax.dot_general(
        a, b, (((1,), (1,)), ((), ())), preferred_element_type=F32
    )


def iota(shape, axis):
    return lax.broadcasted_iota(jnp.int32, shape, axis)


def grid_of(count):
    columns = max(c for c in range(1, math.isqrt(count) + 1) if count % c == 0)
    return count // columns, columns


def kernel(
    sizes,
    x_hbm, wk_hbm, wv_hbm, wf_hbm, wrv_hbm, wrq_hbm, wq_hbm, wog_hbm, wao_hbm, wro_hbm,
    in_gain_hbm, q_gain_hbm, k_gain_hbm, gate_t_hbm, a_gain_hbm,
    slack_hbm, extra_t_hbm, r_gain_hbm,
    mixed_ref, logsum_ref,
    x_v, wkq_v, wfr_v, wvr_v, wog_v, wo_v,
    xn, k_src, q_src, v_src, g_src, k_all, v_all, g_all, ga, q_in, s_buf, w_buf, m_s, l_s,
    o_src, lg_src, o_in, lg_in, mix,
    inner, vq, og, ext, st, up_in, up_out, chain_in, chain_out, incoming, part, send2, recv1, recv2,
    in_gain, q_gain, k_gain, gate_t, a_gain, slack, extra_t, r_gain, rec_part,
    load_sem, k_send, v_send, q_send, g_send, k_recv, v_recv, q_recv, g_recv, k_fwd, v_fwd,
    o_send, o_recv, lg_send, lg_recv,
    st_send, st_recv, up_send, up_recv, chain_send, chain_recv,
    s1_send, s1_recv, s2_send, s2_recv,
):
    nz, ny, ntp = sizes
    n_sp = nz * ny
    rows, width = x_v.shape
    cols = wog_v.shape[1]
    heads = cols // HEAD_DIM
    pairs = cols // LANES
    rec_heads = cols // STATE_ROWS
    chips = ntp // 2
    rb = rows // ntp
    half = rows // 2
    splits = s1_recv.shape[1]
    part_cols = width // splits
    homes = n_sp // (2 * heads)
    members = 2 * homes

    sp, tp = lax.axis_index("sp"), lax.axis_index("tp")
    z, y = sp // ny, sp % ny
    chip, core = tp // 2, tp % 2
    partner = chip * 2 + (1 - core)

    group = sp // homes
    src_core, src_head = group % 2, group // 2
    primary = core == src_core
    member = (sp % homes) * 2 + core
    src_tp = chip * 2 + src_core

    def block_of(j):
        return j * members + (member if j % 2 == 0 else members - 1 - member)

    my_j = sp // members
    my_u = sp % members
    my_member = my_u + (my_j % 2) * (members - 1 - 2 * my_u)
    my_home, my_core = my_member // 2, my_member % 2

    def home_of(i, r):
        return (2 * i + core) * homes + r

    loads = []
    for i, (src, dst) in enumerate((
        (x_hbm, x_v), (wk_hbm, wkq_v.at[:, 0:cols]), (wq_hbm, wkq_v.at[:, cols : 2 * cols]),
        (wf_hbm, wfr_v.at[:, 0:cols]), (wrv_hbm, wfr_v.at[:, cols : 2 * cols]),
        (wv_hbm, wvr_v.at[:, 0:cols]), (wrq_hbm, wvr_v.at[:, cols : 2 * cols]),
        (wog_hbm, wog_v), (wao_hbm, wo_v.at[0:cols, :]),
        (wro_hbm, wo_v.at[cols : 2 * cols, :]),
        (in_gain_hbm, in_gain), (q_gain_hbm, q_gain), (k_gain_hbm, k_gain),
        (gate_t_hbm, gate_t), (a_gain_hbm, a_gain), (slack_hbm, slack),
        (extra_t_hbm, extra_t), (r_gain_hbm, r_gain),
    )):
        loads.append(pltpu.make_async_copy(src, dst, load_sem.at[i - 1 if i in (4, 6) else i]))

    for copy in loads[:1] + loads[10:] + loads[1:3]:
        copy.start()

    def both(ref, i):
        pltpu.make_async_copy(ref, ref, load_sem.at[i]).wait()

    barrier = pltpu.get_barrier_semaphore()

    def greet(where):
        pl.semaphore_signal(barrier, inc=1, device_id=where, device_id_type=MESH)

    for k in range(n_sp):
        if k > 0:
            greet(((sp + k) % n_sp, tp))
        greet(((sp + k) % n_sp, partner))
    for k in range(1, chips):
        greet((sp, ((chip + k) % chips) * 2 + core))

    loads[0].wait()
    for copy in loads[10:]:
        copy.wait()
    for copy in loads[3:5]:
        copy.start()
    xf = x_v[...].astype(F32)
    scale = lax.rsqrt(jnp.mean(xf * xf, axis=-1, keepdims=True) + EPSILON)
    xn[...] = (xf * scale * in_gain[...]).astype(BF16)

    for i in range(heads):
        g_src[i] = gate_t[i : i + 1, :]

    block_ones = jnp.where(
        iota((cols, cols), 0) // HEAD_DIM == iota((cols, cols), 1) // HEAD_DIM, 1.0 / HEAD_DIM, 0.0
    ).astype(BF16)

    def head_norm(v, gain_ref):
        mean = sum(dot(p, block_ones) for p in parts_of(v * v, 2))
        gain = jnp.concatenate([gain_ref[...]] * heads, axis=1)
        return v * lax.rsqrt(mean + EPSILON) * gain

    def by_halves(lanes):
        w = wkq_v[:, lanes]
        return jnp.concatenate([dot(xn[0:half, :], w), dot(xn[half:rows, :], w)], axis=0)

    loads[1].wait()
    keys = head_norm(by_halves(slice(0, cols)), k_gain)
    first_half = iota((half, LANES), 1) < HEAD_DIM
    for p in range(pairs):
        low = keys[0:half, p * LANES : (p + 1) * LANES]
        high = keys[half:rows, p * LANES : (p + 1) * LANES]
        k_src[2 * p] = jnp.where(first_half, low, pltpu.roll(high, HEAD_DIM, 1)).astype(BF16)
        k_src[2 * p + 1] = jnp.where(first_half, pltpu.roll(low, HEAD_DIM, 1), high).astype(BF16)
    def remote(src, dst, send, recv, where):
        return pltpu.make_async_remote_copy(
            src_ref=src, dst_ref=dst, send_sem=send, recv_sem=recv,
            device_id=where, device_id_type=MESH,
        )

    def k_copy(i, r):
        return remote(
            k_src.at[i], k_all.at[sp], k_send, k_recv.at[my_j], (home_of(i, r), tp)
        )

    def v_copy(i, r):
        return remote(
            v_src.at[i], v_all.at[sp], v_send, v_recv.at[my_j], (home_of(i, r), tp)
        )

    def g_copy(i, r, c):
        return remote(
            g_src.at[i], g_all.at[sp], g_send, g_recv, (home_of(i, r), tp if c == 0 else partner)
        )

    def q_copy(i):
        return remote(
            q_src.at[i], q_in.at[my_j], q_send, q_recv.at[my_j],
            (home_of(i, my_home), chip * 2 + my_core),
        )

    def sent(ref, sem):
        remote(ref, ref, sem, g_recv, (sp, partner)).wait_send()

    def landed(ref, sem):
        remote(ref, ref, g_send, sem, (sp, partner)).wait_recv()

    def either(here, act, ref, few, many):
        @pl.when(here)
        def _():
            act(ref.at[0:few])

        @pl.when(jnp.logical_not(here))
        def _():
            act(ref.at[0:many])

    own = primary & (member == my_member)

    turns = [(src_head + k) % heads for k in range(heads)]

    def spread(copies, local):
        for i in turns:
            for r in range(homes):
                @pl.when(home_of(i, r) != sp)
                def _():
                    copies(i, r).start()

                @pl.when(home_of(i, r) == sp)
                def _():
                    local(i)

    def keep_k(i):
        k_all[sp] = k_src[i]

    def keep_v(i):
        v_all[sp] = v_src[i]

    def keep_g(i):
        g_all[sp] = g_src[i]

    def begin():
        pl.semaphore_wait(barrier, 2 * n_sp - 1 + chips - 1)

    def send_keys():
        spread(lambda i, r: g_copy(i, r, 0), keep_g)
        for i in range(heads):
            for r in range(homes):
                g_copy(i, r, 1).start()
        spread(k_copy, keep_k)

    def send_queries():
        for i in turns:
            stays = own & (i == src_head)

            @pl.when(jnp.logical_not(stays))
            def _():
                q_copy(i).start()

            @pl.when(stays)
            def _():
                q_in[my_j] = q_src[i]

    early = z == 0

    @pl.when(jnp.logical_not(early))
    def _():
        begin()
        send_keys()

    loads[2].wait()
    for copy in loads[5:7]:
        copy.start()
    queries = head_norm(by_halves(slice(cols, 2 * cols)), q_gain)
    queries_t = (queries.astype(BF16).astype(F32) * HEAD_DIM ** (-0.5)).T.astype(BF16)
    for i in range(heads):
        q_src[i] = queries_t[i * HEAD_DIM : (i + 1) * HEAD_DIM, :]

    @pl.when(jnp.logical_not(early))
    def _():
        send_queries()

    tri = iota((rows, rows), 0) >= iota((rows, rows), 1)
    tri_b = tri.astype(F32).astype(BF16)
    both(wfr_v, 3)
    for copy in loads[7:10]:
        copy.start()
    fr = dot(xn[...], wfr_v[...])
    share = slack[...] / (1.0 + jnp.exp(fr[:, 0:cols]))
    rec_value = fr[:, cols : 2 * cols]
    run = sum(dot(tri_b, p) for p in parts_of(jnp.log1p(-share), 3))
    ext[...] = jnp.zeros_like(ext)
    ext[0:rec_heads, :] = extra_t[...]
    ext_row = sum(dot_nt(p, tri_b) for p in parts_of(ext[...], 3))
    ext_col = ext_row.T
    last = run[rows - 1 : rows]
    st_rows = STATE_ROWS + 16
    for j in range(rec_heads):
        lanes = slice(j * STATE_ROWS, (j + 1) * STATE_ROWS)
        e_col = ext_col[:, j : j + 1]
        e_row = ext_row[j : j + 1, :]
        e_last = e_row[:, rows - 1 : rows]
        left = share[:, lanes] * jnp.exp(last[:, lanes] - run[:, lanes] + (e_last - e_col))
        st[y, j * st_rows : j * st_rows + STATE_ROWS, :] = dot(
            rec_value[:, lanes].T.astype(BF16), left.astype(BF16)
        ).astype(BF16)
        st[y, j * st_rows + STATE_ROWS : (j + 1) * st_rows, :] = jnp.broadcast_to(
            jnp.exp(last[:, lanes] + e_last), (16, STATE_ROWS)
        ).astype(BF16)

    def st_copy(k):
        return remote(
            st.at[y], st.at[y], st_send, st_recv, (z * ny + (y + k) % ny, tp)
        )

    lifts = (z % 2 == 0) & (z + 1 < nz)

    @pl.when(early)
    def _():
        begin()

    for k in range(1, ny):
        st_copy(k).start()

    @pl.when(early)
    def _():
        send_keys()
        send_queries()

    both(wvr_v, 5)
    vr = dot(xn[...], wvr_v[...])
    values_t = vr[:, 0:cols].T.astype(BF16)
    for i in range(heads):
        v_src[i] = values_t[i * HEAD_DIM : (i + 1) * HEAD_DIM, :]
    spread(v_copy, keep_v)

    rec_query = vr[:, cols : 2 * cols]
    rec_query = rec_query / (1.0 + jnp.exp(-rec_query))
    grown = rec_query * jnp.exp(run)
    for j in range(rec_heads):
        lanes = slice(j * STATE_ROWS, (j + 1) * STATE_ROWS)
        e_col = ext_col[:, j : j + 1]
        e_row = ext_row[j : j + 1, :]
        value = rec_value[:, lanes].astype(BF16)
        scores = dot_nt(
            grown[:, lanes].astype(BF16), (share[:, lanes] * jnp.exp(-run[:, lanes])).astype(BF16)
        )
        fading = jnp.exp(jnp.where(tri, e_col - e_row, -jnp.inf))
        scores = jnp.where(tri, scores * fading, 0.0)
        inner[:, lanes] = dot(scores.astype(BF16), value)
        vq[:, lanes] = (grown[:, lanes] * jnp.exp(e_col)).astype(BF16)

    loads[7].wait()
    gate_out = dot(xn[...], wog_v[...])
    og[...] = gate_out / (1.0 + jnp.exp(-gate_out))

    def up_copy(j):
        return remote(
            up_out.at[j], up_in.at[j], up_send, up_recv.at[j], ((sp + ny) % n_sp, tp)
        )

    def chain_copy(j, d):
        return remote(
            chain_out.at[j], chain_in.at[j], chain_send.at[d - 1], chain_recv.at[j],
            ((sp + d * ny) % n_sp, tp),
        )

    def added(j, k):
        base = j * st_rows
        return (
            st[k, base : base + STATE_ROWS, :].astype(F32),
            st[k, base + STATE_ROWS : base + st_rows, :].astype(F32),
        )

    def states_of_row():
        if ny > 1:
            landed(st.at[0 : ny - 1], st_recv)

    def lift():
        for j in range(rec_heads):
            total, kept = added(j, 0)
            for k in range(1, ny):
                more, decay = added(j, k)
                total, kept = total * decay[0:1] + more, kept * decay
            up_out[j, 0:STATE_ROWS, :] = total.astype(BF16)
            up_out[j, STATE_ROWS:st_rows, :] = kept.astype(BF16)
            up_copy(j).start()

    def advance(received, odd):
        for j in range(rec_heads):
            state = jnp.zeros((STATE_ROWS, STATE_ROWS), F32)
            if received:
                landed(chain_in.at[j], chain_recv.at[j])
                state = chain_in[j].astype(F32)
            if odd:
                landed(up_in.at[j], up_recv.at[j])
                decay = up_in[j, STATE_ROWS:st_rows, :].astype(F32)[0:1]
                state = state * decay + up_in[j, 0:STATE_ROWS, :].astype(F32)
            for k in range(ny):
                @pl.when(y == k)
                def _():
                    incoming[j] = state.astype(BF16)

                if odd or k + 1 < ny:
                    more, decay = added(j, k)
                    state = state * decay[0:1] + more
            if odd:
                chain_out[j] = state.astype(BF16)
                for d in (1, 2):
                    @pl.when(z + d < nz)
                    def _():
                        chain_copy(j, d).start()

    def advance_at(where, received, odd):
        @pl.when(where & (z % 2 == odd))
        def _():
            advance(received, odd)

    states_of_row()

    @pl.when(lifts)
    def _():
        lift()

    advance_at(z < 2, False, 0)

    either(primary, lambda ref: landed(ref, g_recv), g_all, n_sp - 1, n_sp)

    gate_cols = jnp.concatenate(
        [g_all[t, :, h * half : (h + 1) * half] for t in range(n_sp) for h in range(2)], axis=0
    ).T
    gate_parts = jnp.concatenate(
        [p.astype(F32) for p in parts_of(gate_cols, 3)]
        + [jnp.zeros((half, LANES - 6 * n_sp), F32)] * (6 * n_sp < LANES), axis=1
    )
    lane_block = (iota((half, LANES), 1) % (2 * n_sp)) // 2
    for t in range(n_sp):
        ga[t] = jnp.where(lane_block == t, gate_parts, 0.0).astype(BF16)

    def take(ref, fwd, recv, j):
        either(
            primary & (my_j == j), lambda part: landed(part, recv.at[j]), ref,
            members - 1, members,
        )

        @pl.when(primary)
        def _():
            for t in range(j * members, (j + 1) * members):
                remote(ref.at[t], ref.at[t], fwd, recv.at[j], (sp, partner)).start()

    def take_keys(j):
        take(k_all, k_fwd, k_recv, j)

    def take_values(j):
        take(v_all, v_fwd, v_recv, j)

    minus = jnp.where(
        iota((LANES, 2 * rows), 0) % 2 == iota((LANES, 2 * rows), 1) // rows, -1.0, 0.0
    ).astype(BF16)
    ahead = (
        iota((half, 2 * rows), 0) + half * (iota((half, 2 * rows), 1) // rows)
        - iota((half, 2 * rows), 1) % rows
    )
    first = [members * j * (j + 1) // 2 for j in range(heads)]

    def take_query(j):
        @pl.when(jnp.logical_not(own & (my_j == j)))
        def _():
            landed(q_in.at[j], q_recv.at[j])

    def weigh(j):
        q = q_in[j]
        none = jnp.zeros_like(q)
        right = jnp.concatenate(
            [jnp.concatenate([q, none], axis=1), jnp.concatenate([none, q], axis=1), minus], axis=0
        )
        top = None
        for t in range((j + 1) * members):
            s = dot(jnp.concatenate([k_all[t], ga[t]], axis=1), right)
            if t >= j * members:
                s = jnp.where(ahead <= (block_of(j) - t) * rows, s, -jnp.inf)
            s_buf[t] = s
            here = jnp.max(s, axis=0, keepdims=True)
            top = here if top is None else jnp.maximum(top, here)
        top = jnp.maximum(top[:, 0:rows], top[:, rows : 2 * rows])
        m_s[j] = top
        top = jnp.concatenate([top, top], axis=1)
        total = None
        for t in range((j + 1) * members):
            w = jnp.exp(s_buf[t] - top)
            here = jnp.sum(w, axis=0, keepdims=True)
            total = here if total is None else total + here
            w = w.astype(BF16)
            w_buf[first[j] + t, 0:half, :] = w[:, 0:rows]
            w_buf[first[j] + t, half:rows, :] = w[:, rows : 2 * rows]
        l_s[j] = total[:, 0:rows] + total[:, rows : 2 * rows]

    def o_copy(j):
        return remote(
            o_src.at[j], o_in.at[src_head], o_send, o_recv, (block_of(j), src_tp)
        )

    def lg_copy(j):
        return remote(
            lg_src.at[j], lg_in.at[src_head], lg_send, lg_recv, (block_of(j), src_tp)
        )

    def finish(j):
        n = (j + 1) * members
        summed = [
            sum(dot(v_all[t], w_buf[first[j] + t]) for t in range(u, n, 2)) for u in range(2)
        ]
        out = (summed[0] + summed[1]) / l_s[j]
        mean = jnp.mean(out * out, axis=0, keepdims=True)
        o_src[j] = (out * lax.rsqrt(mean + EPSILON)).astype(BF16)
        lg_src[j] = m_s[j] + jnp.log(l_s[j])

    def give(j):
        kept = own & (my_j == j)

        @pl.when(jnp.logical_not(kept))
        def _():
            o_copy(j).start()
            lg_copy(j).start()

        @pl.when(kept)
        def _():
            o_in[src_head] = o_src[j]
            lg_in[src_head] = lg_src[j]

    def each(jobs, *acts):
        for act in acts:
            for j in jobs:
                act(j)

    at = max(heads - 2, 1)
    each(range(at), take_keys, take_query, weigh)
    each(range(at, heads), take_keys, take_query)
    advance_at(z < 2, False, 1)
    each((0,), take_values, finish, give)
    each(range(at, heads), weigh)
    each(range(1, heads - 1), take_values, finish, give)
    each((heads - 1,), take_values, finish, give)
    advance_at(z >= 2, True, 0)
    advance_at(z >= 2, True, 1)

    for j in range(rec_heads):
        lanes = slice(j * STATE_ROWS, (j + 1) * STATE_ROWS)
        out = inner[:, lanes] + dot_nt(vq[:, lanes], incoming[j])
        mean = jnp.mean(out * out, axis=-1, keepdims=True)
        out = out * lax.rsqrt(mean + EPSILON) * r_gain[:, lanes] * og[:, lanes]
        mix[:, cols + j * STATE_ROWS : cols + (j + 1) * STATE_ROWS] = out.astype(BF16)
    loads[9].wait()
    rec_part[...] = dot(mix[:, cols : 2 * cols], wo_v[cols : 2 * cols, :])
    loads[8].wait()

    either(own, lambda ref: landed(ref, o_recv), o_in, heads - 1, heads)
    either(own, lambda ref: landed(ref, lg_recv), lg_in, heads - 1, heads)

    for i in range(heads):
        logsum_ref[i : i + 1, :] = lg_in[i] + gate_t[i : i + 1, :]
    attn_t = jnp.concatenate([o_in[i].astype(F32) for i in range(heads)], axis=0)
    mix[:, 0:cols] = (attn_t.T * a_gain[...]).astype(BF16)

    def rows_of(which_chip, which_core):
        return pl.ds(pl.multiple_of((which_chip * 2 + which_core) * rb, rb), rb)

    def columns(q):
        return slice(q * part_cols, (q + 1) * part_cols)

    def within(j, q):
        return pltpu.make_async_remote_copy(
            src_ref=part.at[q, rows_of(j, 1 - core)], dst_ref=recv1.at[j, q],
            send_sem=s1_send, recv_sem=s1_recv.at[j, q], device_id=(sp, partner),
            device_id_type=MESH,
        )

    def between(j, q):
        return pltpu.make_async_remote_copy(
            src_ref=send2.at[j, q], dst_ref=recv2.at[chip, q], send_sem=s2_send,
            recv_sem=s2_recv.at[chip, q], device_id=(sp, j * 2 + core), device_id_type=MESH,
        )

    order = [(chip + k) % chips for k in range(1, chips)]

    def chip_sum(j, q):
        within(j, q).wait_recv()
        return part[q, rows_of(j, core), :].astype(F32) + recv1[j, q].astype(F32)

    def send_sums(q):
        for j in order:
            send2[j, q] = chip_sum(j, q).astype(BF16)
            between(j, q).start()

    def partial_of(j, q):
        at = pl.ds(pl.multiple_of(j * 2 * rb, 2 * rb), 2 * rb)
        part[q, at, :] = (
            dot(mix[at, 0:cols], wo_v[0:cols, columns(q)]) + rec_part[at, columns(q)]
        ).astype(BF16)
        within(j, q).start()

    for q in range(splits):
        for j in order:
            partial_of(j, q)
        if q > 0:
            send_sums(q - 1)
    send_sums(splits - 1)
    for q in range(splits):
        partial_of(chip, q)
    for q in range(splits):
        total = chip_sum(chip, q)
        for j in order:
            pltpu.make_async_remote_copy(
                src_ref=send2.at[j, q], dst_ref=recv2.at[j, q], send_sem=s2_send,
                recv_sem=s2_recv.at[j, q], device_id=(sp, partner), device_id_type=MESH,
            ).wait_recv()
            total = total + recv2[j, q].astype(F32)
        mixed_ref[:, columns(q)] = total.astype(BF16)

    sent(recv1, s1_send)
    if chips > 1:
        sent(recv2.at[0 : chips - 1], s2_send)
    if ny > 1:
        sent(st.at[0 : ny - 1], st_send)

    @pl.when(lifts)
    def _():
        sent(up_out, up_send)

    for d in (1, 2):
        @pl.when((z % 2 == 1) & (z + d < nz))
        def _():
            sent(chain_out, chain_send.at[d - 1])

    copies = heads * homes
    either(primary, lambda ref: sent(ref, k_send), k_all, copies - 1, copies)
    either(primary, lambda ref: sent(ref, v_send), v_all, copies - 1, copies)
    either(primary, lambda ref: sent(ref, g_send), g_all, n_sp - 1, n_sp)
    either(own, lambda ref: sent(ref, q_send), q_in, heads - 1, heads)
    either(own, lambda ref: sent(ref, o_send), o_in, heads - 1, heads)
    either(own, lambda ref: sent(ref, lg_send), lg_in, heads - 1, heads)

    @pl.when(primary)
    def _():
        sent(k_all, k_fwd)
        sent(v_all, v_fwd)


def leave(mixed_v, log_sum_v, mixed_hbm, log_sum_hbm, sem):
    copies = (
        pltpu.make_async_copy(mixed_v, mixed_hbm, sem.at[0]),
        pltpu.make_async_copy(log_sum_v, log_sum_hbm, sem.at[1]),
    )
    for copy in copies:
        copy.start()
    for copy in copies:
        copy.wait()


def body(
    n_sp, n_tp,
    layer_input_rows, input_norm_gain, query_weight, key_weight, value_weight, query_norm_gain,
    key_norm_gain, cumulative_gate, attention_norm_gain, recurrence_query_weight, forget_weight,
    recurrence_value_weight, output_gate_weight, gate_lower_slack, extra_log_decay,
    recurrence_norm_gain, attention_output_weight, recurrence_output_weight,
):
    nz, ny = grid_of(n_sp)
    rows, width = layer_input_rows.shape
    cols = query_weight.shape[1]
    heads, pairs, rec_heads = cols // HEAD_DIM, cols // LANES, cols // STATE_ROWS
    rb, chips = rows // n_tp, n_tp // 2
    half = rows // 2
    homes = n_sp // (2 * heads)
    blocks = 2 * homes * heads * (heads + 1) // 2
    splits = math.gcd(width // LANES, 4)
    weight = pltpu.VMEM((width, cols), BF16)
    two_weights = pltpu.VMEM((width, 2 * cols), BF16)
    dma = pltpu.SemaphoreType.DMA
    any_space = pl.BlockSpec(memory_space=pl.ANY)
    vmem = pl.BlockSpec(memory_space=pltpu.VMEM)
    mixed, log_sum = pl.pallas_call(
        functools.partial(kernel, (nz, ny, n_tp)),
        name="mixer",
        out_shape=(
            jax.ShapeDtypeStruct((rb, width), BF16),
            jax.ShapeDtypeStruct((heads, rows), F32),
        ),
        in_specs=[any_space] * 18,
        out_specs=(vmem, vmem),
        scratch_shapes=[
            pltpu.VMEM((rows, width), BF16),
            *([two_weights] * 3), weight, pltpu.VMEM((2 * cols, width), BF16),
            pltpu.VMEM((rows, width), BF16),
            pltpu.VMEM((heads, half, LANES), BF16),
            pltpu.VMEM((heads, HEAD_DIM, rows), BF16),
            pltpu.VMEM((heads, HEAD_DIM, rows), BF16),
            pltpu.VMEM((heads, 1, rows), F32),
            pltpu.VMEM((n_sp, half, LANES), BF16),
            pltpu.VMEM((n_sp, HEAD_DIM, rows), BF16),
            pltpu.VMEM((n_sp, 1, rows), F32),
            pltpu.VMEM((n_sp, half, LANES), BF16),
            pltpu.VMEM((heads, HEAD_DIM, rows), BF16),
            pltpu.VMEM((n_sp, half, 2 * rows), F32),
            pltpu.VMEM((blocks, rows, rows), BF16),
            pltpu.VMEM((heads, 1, rows), F32),
            pltpu.VMEM((heads, 1, rows), F32),
            pltpu.VMEM((heads, HEAD_DIM, rows), BF16),
            pltpu.VMEM((heads, 1, rows), F32),
            pltpu.VMEM((heads, HEAD_DIM, rows), BF16),
            pltpu.VMEM((heads, 1, rows), F32),
            pltpu.VMEM((rows, 2 * cols), BF16),
            pltpu.VMEM((rows, cols), F32),
            pltpu.VMEM((rows, cols), BF16),
            pltpu.VMEM((rows, cols), F32),
            pltpu.VMEM((8, rows), F32),
            pltpu.VMEM((ny, rec_heads * (STATE_ROWS + 16), STATE_ROWS), BF16),
            *([pltpu.VMEM((rec_heads, STATE_ROWS + 16, STATE_ROWS), BF16)] * 2),
            *([pltpu.VMEM((rec_heads, STATE_ROWS, STATE_ROWS), BF16)] * 3),
            pltpu.VMEM((splits, rows, width // splits), BF16),
            *([pltpu.VMEM((chips, splits, rb, width // splits), BF16)] * 3),
            *([pltpu.VMEM((1, n), F32) for n in (width, HEAD_DIM, HEAD_DIM)]),
            pltpu.VMEM((heads, rows), F32),
            pltpu.VMEM((1, cols), F32),
            pltpu.VMEM((1, cols), F32),
            pltpu.VMEM((rec_heads, rows), F32),
            pltpu.VMEM((1, cols), F32),
            pltpu.VMEM((rows, width), F32),
            dma((18,)),
            dma, dma, dma, dma,
            *([dma((heads,))] * 3), dma, dma, dma,
            dma, dma, dma, dma,
            dma, dma, dma, dma((rec_heads,)), dma((2,)), dma((rec_heads,)),
            dma, dma((chips, splits)), dma, dma((chips, splits)),
        ],
        compiler_params=pltpu.CompilerParams(
            collective_id=0, has_side_effects=True, vmem_limit_bytes=48 * 1024 * 1024
        ),
    )(*(pltpu.with_memory_space_constraint(a, pltpu.HBM) for a in (
        layer_input_rows, key_weight, value_weight, forget_weight, recurrence_value_weight,
        recurrence_query_weight, query_weight, output_gate_weight, attention_output_weight,
        recurrence_output_weight,
        input_norm_gain.reshape(1, -1), query_norm_gain.reshape(1, -1),
        key_norm_gain.reshape(1, -1), cumulative_gate.T, attention_norm_gain.reshape(1, -1),
        gate_lower_slack.reshape(1, -1), extra_log_decay.T, recurrence_norm_gain.reshape(1, -1),
        )))
    mixed, log_sum = pl.pallas_call(
        leave,
        name="leave",
        out_shape=(
            jax.ShapeDtypeStruct((rb, width), BF16),
            jax.ShapeDtypeStruct((heads, rows), F32),
        ),
        in_specs=[vmem] * 2,
        out_specs=(any_space, any_space),
        scratch_shapes=[dma((2,))],
        compiler_params=pltpu.CompilerParams(vmem_limit_bytes=4 * 1024 * 1024),
    )(mixed, log_sum)
    return mixed, log_sum.T


def solution(mesh):
    return jax.shard_map(
        functools.partial(body, mesh.shape["sp"], mesh.shape["tp"]),
        mesh=mesh,
        in_specs=(
            P("sp", None),
            P(),
            P(None, "tp"),
            P(None, "tp"),
            P(None, "tp"),
            P(),
            P(),
            P("sp", "tp"),
            P("tp"),
            P(None, "tp"),
            P(None, "tp"),
            P(None, "tp"),
            P(None, "tp"),
            P("tp"),
            P("sp", "tp"),
            P("tp"),
            P("tp", None),
            P("tp", None),
        ),
        out_specs=(P(("sp", "tp"), None), P("sp", "tp")),
        check_vma=False,
    )
```
